256 devices in a mesh: ep: 128 (over z, y, x), tp: 2 (over core).
Axes of the slice: x: 4, y: 4, z: 8, core: 2. Of those that a mesh axis runs over, the one named last changes fastest.
Arguments:
- tokens: bfloat16 [2048, 2048], P('ep', 'tp'), may hold values from -6 to 6
- state: float32 [2048, 4, 128, 128], P('ep', 'tp'), may hold values from -4 to 4
- norm_mix: float32 [2048], replicated, may hold values from 0.1 to 1.9
- w_query: bfloat16 [2048, 512], P(None, 'tp'), may hold values from -0.125 to 0.125
- w_key: bfloat16 [2048, 512], P(None, 'tp'), may hold values from -0.125 to 0.125
- w_value: bfloat16 [2048, 512], P(None, 'tp'), may hold values from -0.125 to 0.125
- w_out: bfloat16 [512, 2048], P('tp'), may hold values from -0.25 to 0.25
- norm_ffn: float32 [2048], P('tp'), may hold values from 0.1 to 1.9
- gate_vector: bfloat16 [2048], P('tp'), may hold values from -0.125 to 0.125
- dense_gate: bfloat16 [2048, 2816], P('tp', 'ep'), may hold values from -0.125 to 0.125
- dense_up: bfloat16 [2048, 2816], P('tp', 'ep'), may hold values from -0.125 to 0.125
- dense_down: bfloat16 [2816, 2048], P('ep', 'tp'), may hold values from -0.109375 to 0.109375
- exp_gate: bfloat16 [128, 2048, 176], P('ep', None, 'tp'), may hold values from -0.125 to 0.125
- exp_up: bfloat16 [128, 2048, 176], P('ep', None, 'tp'), may hold values from -0.125 to 0.125
- exp_down: bfloat16 [128, 176, 2048], P('ep', 'tp'), may hold values from -0.109375 to 0.109375
- routes: int32 [2048, 2], P('ep'), may hold values from 0 to 7, all different within a row; in each aligned block of 16 rows (0 to 15, 16 to 31, ...) at most 5 rows name the same one
- route_w: bfloat16 [2048, 2], P('ep'), may hold values from 0.099609375 to 1
Outputs:
- mixed: bfloat16 [2048, 2048], P('ep', 'tp')
- new_state: float32 [2048, 4, 128, 128], P('ep', 'tp')
The draws below stay inside these ranges and needn't reach their ends.
Inputs may be any that keep to these rules, and one draw needn't show every extreme that they name: `routes`: each row names 2 different experts. Within the rows of one device (aligned blocks of 16 rows) no expert is named by more than 5 rows, a bound that some blocks reach.
All inputs are finite; a program needn't handle non-finite values.
Results may differ from the reference program's by a relative error of at most 0.014.
Values may be sent and summed in bfloat16 or wider, within the bound.
A program may use at most 128 MiB of HBM per device.

```python
import math
import jax
import jax.numpy as jnp
import numpy as np
from jax import lax

D = 2048
HEADS = 4
HEAD = 128
FF = 2816
FF_D = 2816
EXPERTS = 8
TOPK = 2
SEQ_DEV = 16
CAP = 5
E_SPLIT = 16
TOKENS = 2048
N_EP = 128
N_TP = 2


def levels(own_key, shape, pieces, low, largest):
    level = 1.0
    for dim, blocks in pieces:
        draws = jax.random.uniform(jax.random.fold_in(jax.random.fold_in(own_key, 6), dim), (blocks,), jnp.float32, low / len(pieces), largest / len(pieces))
        level = level * jnp.repeat(jnp.exp(draws), shape[dim] // blocks).reshape((-1,) + (1,) * (len(shape) - 1 - dim))
    return level


def shared_out(own_key, own, number, rows, count, top, reach, lean):
    order = jax.random.permutation(own_key, count)
    packed, usual = shares(count, rows * top, reach, lean, True), shares(count, rows * top, reach, lean, False)
    places = jnp.arange(count)

    def named(lengths, turn):
        used = int((lengths > 0).sum())
        fixed = max(1, used // 4)
        moved = fixed + (places - fixed + turn * (used - fixed)) % max(1, count - fixed)
        return jnp.zeros((count,), jnp.int32).at[order[jnp.where(places < fixed, places, moved)]].set(jnp.asarray(lengths, jnp.int32))

    lengths = jnp.where(number % 4 == 0, named(packed, number // 4), named(usual, number - number // 4 - 1))
    mixed = jax.random.permutation(jax.random.fold_in(own, 3), count)
    donor, taker = mixed[0:count // 2 * 2:2], mixed[1:count // 2 * 2:2]
    slack = jnp.minimum(lengths[donor] - 1, reach - lengths[taker]) // 2
    slack = jnp.where((donor == order[0]) | (taker == order[0]) | (lengths[taker] == 0), 0, jnp.maximum(slack, 0))
    moved = jax.random.randint(jax.random.fold_in(own, 4), (count // 2,), 0, 1 << 20) % (slack + 1)
    lengths = lengths.at[donor].add(-moved).at[taker].add(moved)
    labels = jnp.searchsorted(jnp.cumsum(lengths), jnp.arange(rows * top), side="right").astype(jnp.int32)
    listing = labels.reshape(top, rows).T
    listing = listing[jax.random.permutation(jax.random.fold_in(own, 1), rows)]
    turn = jax.random.randint(jax.random.fold_in(own, 2), (rows, 1), 0, top)
    return jnp.take_along_axis(listing, (jnp.arange(top)[None, :] + turn) % top, axis=1)


def shares(number_of, total, bound, slope, full):
    loads = [(1 << 20) // math.isqrt(grade ** slope) + 1 for grade in range(1, number_of + 1)]
    largest = bound if full else min(bound, max(-(-total // number_of), total * loads[0] // sum(loads)))
    least = 1 if total - largest >= number_of - 1 else 0
    counts, spare = [largest] + [least] * (number_of - 1), total - largest - least * (number_of - 1)
    while spare > 0:
        free = [i for i in range(1, number_of) if counts[i] < largest] or [i for i in range(1, number_of) if counts[i] < bound]
        whole, left = sum([loads[i] for i in free]), spare
        for i in free:
            extra = min(bound - counts[i], max(1, left * loads[i] // whole), spare)
            counts[i] = counts[i] + extra
            spare = spare - extra
    return np.array(counts)


def gaussian(own_key, dims, scale, bound, cuts=(), kind=jnp.bfloat16):
    level = levels(own_key, dims, cuts, -0.22, 0.18) if cuts else 1.0
    entries = jax.random.normal(own_key, dims, jnp.float32) * scale * level
    return jnp.minimum(jnp.maximum(entries, -bound), bound).astype(kind)


def setup_inputs(seed: int = 0) -> dict:
    seeds = jax.random.split(jax.random.key(seed), 18)
    tokens = gaussian(seeds[0], (TOKENS, D), 1.0, 6.0, ((0, 128), (1, 2)))
    state = gaussian(seeds[1], (TOKENS, HEADS, HEAD, HEAD), 0.5, 4.0, ((0, 128), (1, 2)), jnp.float32)
    norm_mix = jnp.clip(1.0 + 0.18 * jax.random.normal(seeds[2], (D,), jnp.float32), 0.1, 1.9)
    w_query = gaussian(seeds[3], (D, HEADS * HEAD), D ** -0.5, 0.125, ((1, 2),))
    w_key = gaussian(seeds[4], (D, HEADS * HEAD), D ** -0.5, 0.125, ((1, 2),))
    w_value = gaussian(seeds[5], (D, HEADS * HEAD), D ** -0.5, 0.125, ((1, 2),))
    w_out = gaussian(seeds[6], (HEADS * HEAD, D), (HEADS * HEAD) ** -0.5, 0.25, ((0, 2),))
    norm_ffn = jnp.clip(1.0 + 0.18 * jax.random.normal(seeds[7], (D,), jnp.float32), 0.1, 1.9)
    gate_vector = gaussian(seeds[8], (D,), D ** -0.5, 0.125, ((0, 2),))
    dense_gate = gaussian(seeds[9], (D, FF_D), D ** -0.5, 0.125, ((0, 2), (1, 128)))
    dense_up = gaussian(seeds[10], (D, FF_D), D ** -0.5, 0.125, ((0, 2), (1, 128)))
    dense_down = gaussian(seeds[11], (FF_D, D), FF_D ** -0.5, 0.109375, ((0, 128), (1, 2)))
    exp_gate = gaussian(seeds[12], (EXPERTS * E_SPLIT, D, FF // E_SPLIT), D ** -0.5, 0.125, ((0, 128), (2, 2)))
    exp_up = gaussian(seeds[13], (EXPERTS * E_SPLIT, D, FF // E_SPLIT), D ** -0.5, 0.125, ((0, 128), (2, 2)))
    exp_down = gaussian(seeds[14], (EXPERTS * E_SPLIT, FF // E_SPLIT, D), FF ** -0.5, 0.109375, ((0, 128), (1, 2)))
    routes_keys = jax.random.split(jax.random.fold_in(seeds[15], 1), TOKENS // SEQ_DEV)
    routes_turns = jax.random.permutation(jax.random.fold_in(seeds[15], 3), TOKENS // SEQ_DEV)
    routes = jax.vmap(lambda own, number: shared_out(jax.random.fold_in(seeds[15], 2), own, number, SEQ_DEV, EXPERTS, TOPK, CAP, 1))(routes_keys, routes_turns).reshape((TOKENS, TOPK))
    route_w = jnp.clip(0.099609375 + 0.9003906 * jax.random.uniform(seeds[16], (TOKENS, TOPK), jnp.float32) ** levels(seeds[16], (TOKENS, TOPK), ((0, 128),), -0.2, 0.2), 0.099609375, 1.0).astype(jnp.bfloat16)
    return dict(tokens=tokens, state=state, norm_mix=norm_mix, w_query=w_query, w_key=w_key, w_value=w_value, w_out=w_out, norm_ffn=norm_ffn, gate_vector=gate_vector, dense_gate=dense_gate, dense_up=dense_up, dense_down=dense_down, exp_gate=exp_gate, exp_up=exp_up, exp_down=exp_down, routes=routes, route_w=route_w)


epsilon = 1e-06

def reference(tokens, state, norm_mix, w_query, w_key, w_value, w_out, norm_ffn, gate_vector, dense_gate, dense_up, dense_down, exp_gate, exp_up, exp_down, routes, route_w):
    highest = lax.Precision.HIGHEST
    tok_f = tokens.astype(jnp.float32)
    normed = (tok_f * lax.rsqrt(lax.optimization_barrier(jnp.mean(tok_f * tok_f, axis=1, keepdims=True)) + epsilon) * norm_mix).astype(jnp.bfloat16)
    query = jnp.dot(normed, w_query, preferred_element_type=jnp.float32).astype(jnp.bfloat16)
    key_rows = jnp.dot(normed, w_key, preferred_element_type=jnp.float32).astype(jnp.bfloat16)
    value_rows = jnp.dot(normed, w_value, preferred_element_type=jnp.float32).astype(jnp.bfloat16)
    row_count = tokens.shape[0]
    query3 = query.astype(jnp.float32).reshape(row_count, HEADS, HEAD)
    key3 = key_rows.astype(jnp.float32).reshape(row_count, HEADS, HEAD) * HEAD ** (-0.5)
    value3 = value_rows.astype(jnp.float32).reshape(row_count, HEADS, HEAD)
    head_ids = jnp.arange(HEADS, dtype=jnp.float32)
    decay = 1.0 - jnp.exp2(-3.0 - 2.0 * head_ids)
    new_state = decay[None, :, None, None] * state + jnp.einsum('shd,she->shde', key3, value3, precision=highest)
    read = jnp.einsum('shd,shde->she', query3, new_state, precision=highest)
    centre = lax.optimization_barrier(jnp.mean(read, axis=2, keepdims=True))
    spread = lax.optimization_barrier(jnp.mean(jnp.square(read - centre), axis=2, keepdims=True))
    heads_out = ((read - centre) * lax.rsqrt(spread + epsilon)).astype(jnp.bfloat16).reshape(row_count, HEADS * HEAD)
    group_cols = HEADS * HEAD // N_TP
    mix_sum = jnp.zeros((row_count, D), jnp.float32)
    for group in range(N_TP):
        lower = group * group_cols
        partial_value = jnp.dot(heads_out[:, lower:lower + group_cols], w_out[lower:lower + group_cols], preferred_element_type=jnp.float32)
        rounded = lax.optimization_barrier(partial_value.astype(jnp.bfloat16))
        mix_sum = mix_sum + rounded.astype(jnp.float32)
    after = (tok_f + mix_sum).astype(jnp.bfloat16)
    after_f = after.astype(jnp.float32)
    normed2 = (after_f * lax.rsqrt(lax.optimization_barrier(jnp.mean(after_f * after_f, axis=1, keepdims=True)) + epsilon) * norm_ffn).astype(jnp.bfloat16)
    dense_pre = jnp.dot(normed2, dense_gate, preferred_element_type=jnp.float32)
    up_pre = jnp.dot(normed2, dense_up, preferred_element_type=jnp.float32)
    logit = jnp.dot(normed2, gate_vector, preferred_element_type=jnp.float32)
    dense_hidden = (jax.nn.sigmoid(logit)[:, None] * jax.nn.silu(dense_pre) * up_pre).astype(jnp.bfloat16)
    dense = jnp.dot(dense_hidden, dense_down, preferred_element_type=jnp.float32)
    group_size = N_EP // EXPERTS
    part_ff = exp_gate.shape[2]
    gate_all = exp_gate.reshape(EXPERTS, group_size, D, part_ff).transpose(0, 2, 1, 3).reshape(EXPERTS, D, group_size * part_ff)
    up_all = exp_up.reshape(EXPERTS, group_size, D, part_ff).transpose(0, 2, 1, 3).reshape(EXPERTS, D, group_size * part_ff)
    down_all = exp_down.reshape(EXPERTS, group_size * part_ff, D)
    onehot = (routes[:, :, None] == jnp.arange(EXPERTS, dtype=jnp.int32)[None, None, :]).astype(jnp.float32)
    member = lax.optimization_barrier(jnp.sum(onehot, axis=1))
    weight = lax.optimization_barrier(jnp.sum(onehot * route_w.astype(jnp.float32)[:, :, None], axis=1))
    member_b = member.reshape(N_EP, SEQ_DEV, EXPERTS)
    slot_b = jnp.cumsum(member_b, axis=1) - member_b
    weight_b = weight.reshape(N_EP, SEQ_DEV, EXPERTS)
    rows_b = normed2.astype(jnp.float32).reshape(N_EP, SEQ_DEV, D)
    slot_ids = jnp.arange(CAP, dtype=jnp.float32)

    def one_expert(total, inputs):
        gate_w, up_w, down_w, pick, place, scale = inputs
        select = pick[:, None, :] * (place[:, None, :] == slot_ids[None, :, None]).astype(jnp.float32)
        chosen = jnp.einsum('ncr,nrd->ncd', select, rows_b, precision=highest).astype(jnp.bfloat16).reshape(N_EP * CAP, D)
        gate_pre = jnp.dot(chosen, gate_w, preferred_element_type=jnp.float32)
        up_part = jnp.dot(chosen, up_w, preferred_element_type=jnp.float32)
        hidden = (jax.nn.silu(gate_pre) * up_part).astype(jnp.bfloat16)
        result = jnp.dot(hidden, down_w, preferred_element_type=jnp.float32).reshape(N_EP, CAP, D)
        contrib = jnp.einsum('ncr,ncd->nrd', select * scale[:, None, :], result, precision=highest)
        return (total + contrib, None)
    moe, _ = lax.scan(one_expert, jnp.zeros((N_EP, SEQ_DEV, D), jnp.float32), (gate_all, up_all, down_all, member_b.transpose(2, 0, 1), slot_b.transpose(2, 0, 1), weight_b.transpose(2, 0, 1)))
    mixed = (after_f + moe.reshape(row_count, D) + dense).astype(jnp.bfloat16)
    return (mixed, new_state)
```

```python
import jax
import jax.numpy as jnp
from jax import lax
from jax.experimental import pallas as pl
from jax.experimental.pallas import tpu as pltpu
from jax.sharding import Mesh
from jax.sharding import PartitionSpec as P

EP = ("ep_0", "ep_1", "ep_2")
Z, Y, X = EP
MESH = pl.DeviceIdType.MESH
SLOT = 8
CAP = 5
F32 = jnp.float32
BF16 = jnp.bfloat16
epsilon = 1e-06
COPIES = 120


def iota(shape, dim):
    return lax.broadcasted_iota(jnp.int32, shape, dim)


def dot(a, b):
    return jnp.dot(a, b, preferred_element_type=F32)


def dot_nt(a, b):
    return lax.dot_general(a, b, (((1,), (1,)), ((), ())), preferred_element_type=F32)


def dot_tn(a, b):
    return lax.dot_general(a, b, (((0,), (0,)), ((), ())), preferred_element_type=F32)


def silu(v):
    return v / (1.0 + jnp.exp(-v))


def pack_matrices(c):
    def slots(row, col):
        in_a = (row < 16) & (col == (row // 4) * SLOT + row % 4)
        in_b = (row >= 16) & (row < 20) & (col == (row - 16) * SLOT + 4)
        return jnp.where(in_a | in_b, 1.0, 0.0).astype(BF16)

    def own(row, col):
        return jnp.where((row >= 20) & (row < 28) & (col == c * 8 + row - 20), 1.0, 0.0).astype(BF16)

    return (
        slots(iota((32, 32), 0), iota((32, 32), 1)),
        own(iota((32, 16), 0), iota((32, 16), 1)),
        slots(iota((32, 32), 1), iota((32, 32), 0)),
        own(iota((16, 32), 1), iota((16, 32), 0)),
    )


def kernel(
    tokens,
    norm_mix,
    norm_ffn,
    gate_vec,
    routes,
    route_w,
    dgate,
    dup,
    ddown,
    state,
    w_query,
    w_key,
    w_value,
    w_out,
    egate,
    eup,
    edown,
    mixed,
    new_state,
    wq,
    wk,
    wv,
    wo,
    st,
    read,
    tok_p,
    nf_p,
    gv_p,
    mix_o,
    mix_p,
    we,
    wd,
    disp,
    zrecv,
    xs,
    outs,
    opp_q,
    fin_q,
    tsend,
    opp_p,
    fin_p,
    rbuf,
    ret,
    dsend,
    drecv,
    local_sem,
    send_sem,
    recv_sem,
    ret_send,
    ret_recv,
):
    z, y, x, c = (lax.axis_index(a) for a in (Z, Y, X, "tp"))
    first = c == 0
    size = {Z: 8, Y: 4, X: 4}
    at = {Z: z, Y: y, X: x}
    used = [0]

    def shift(axis, by):
        return {axis: lax.rem(at[axis] + by + size[axis], size[axis])}

    partner = {"tp": 1 - c}

    def remote(src, dst, device):
        n = used[0]
        used[0] += 1
        return pltpu.make_async_remote_copy(
            src_ref=src,
            dst_ref=dst,
            send_sem=send_sem.at[n],
            recv_sem=recv_sem.at[n],
            device_id=device,
            device_id_type=MESH,
        )

    def started(src, dst, device):
        copy = remote(src, dst, device)
        copy.start()
        return copy

    def halves(own, other):
        return jnp.where(first, own, other), jnp.where(first, other, own)

    loads = []
    for n, (src, dst) in enumerate(
        [
            (w_query, wq),
            (w_key, wk),
            (w_value, wv),
            (state, st),
            (w_out, wo),
            (egate, we.at[0, pl.ds(0, 88)]),
            (eup, we.at[1, pl.ds(0, 88)]),
            (edown, we.at[2, pl.ds(0, 88)]),
        ]
    ):
        copy = pltpu.make_async_copy(src, dst, local_sem.at[n])
        copy.start()
        loads.append(copy)

    for t, ref in enumerate((dgate, dup, ddown)):
        block = jnp.concatenate([ref[...].astype(F32), jnp.zeros((2, 1024), F32)], axis=0)
        wd[t, pl.ds(c, 1), pl.ds(0, 24), :] = block.astype(BF16)[None]

    barrier = pltpu.get_barrier_semaphore()
    peers = [partner]
    for by in range(1, 8):
        for core in (c, 1 - c):
            peers.append({**shift(Z, by), "tp": core})
    for axis in (Y, X):
        peers += [shift(axis, 1), shift(axis, -1)]
    for peer in peers:
        pl.semaphore_signal(barrier, inc=1, device_id=peer, device_id_type=MESH)
    pl.semaphore_wait(barrier, len(peers))

    pair = [started(tokens, tok_p, partner), started(norm_ffn, nf_p, partner), started(gate_vec, gv_p, partner)]

    def wd_slot(n):
        return wd.at[:, pl.ds(c, 1), pl.ds(24 * n, 24), :]

    ring = {}
    ring[1] = started(wd_slot(0), wd_slot(1), shift(Z, 1))
    ring[7] = started(wd_slot(0), wd_slot(7), shift(Z, -1))
    swap = [started(src, we.at[t, pl.ds(88, 88)], partner) for t, src in enumerate((egate, eup, edown))]

    for copy in pair:
        copy.wait_recv()
    lo, hi = halves(tokens[...].astype(F32), tok_p[...].astype(F32))
    full = jnp.concatenate([lo, hi], axis=1)
    mean = jnp.sum(full * full, axis=1, keepdims=True) / 2048.0
    normed = (full * lax.rsqrt(mean + epsilon) * norm_mix[...]).astype(BF16)
    for copy in loads[:3]:
        copy.wait()
    query = dot(normed, wq[...]).astype(BF16).astype(F32)
    key = dot(normed, wk[...]).astype(BF16).astype(F32) * 128 ** (-0.5)
    value = dot(normed, wv[...]).astype(BF16).astype(F32)
    blank = jnp.zeros((112, 256), F32)
    query_t = jnp.concatenate([query, blank], axis=0).T
    key_t = jnp.concatenate([key, blank], axis=0).T
    loads[3].wait()
    for h in range(2):
        decay = jnp.where(first, 1.0 - 2.0 ** (-3.0 - 2.0 * h), 1.0 - 2.0 ** (-7.0 - 2.0 * h))
        for s in range(16):
            k_col = key_t[h * 128 : (h + 1) * 128, s : s + 1]
            q_col = query_t[h * 128 : (h + 1) * 128, s : s + 1]
            v_row = value[s : s + 1, h * 128 : (h + 1) * 128]
            new = decay * st[s, h] + k_col * v_row
            st[s, h] = new
            read[s : s + 1, h * 128 : (h + 1) * 128] = jnp.sum(q_col * new, axis=0, keepdims=True)
    keep = pltpu.make_async_copy(st, new_state, local_sem.at[8])
    keep.start()
    heads = []
    for h in range(2):
        part = read[:, h * 128 : (h + 1) * 128]
        centre = jnp.mean(part, axis=1, keepdims=True)
        spread = jnp.mean(jnp.square(part - centre), axis=1, keepdims=True)
        heads.append(((part - centre) * lax.rsqrt(spread + epsilon)).astype(BF16))
    loads[4].wait()
    mix = dot(heads[0], wo[0:128, :]) + dot(heads[1], wo[128:256, :])
    mix_o[...] = mix.astype(BF16)
    mix_copy = started(mix_o, mix_p, partner)

    ring[1].wait_recv()
    ring[2] = started(wd_slot(1), wd_slot(2), shift(Z, 1))
    ring[7].wait_recv()
    ring[6] = started(wd_slot(7), wd_slot(6), shift(Z, -1))

    block = iota((64, 16), 0)
    expert = lax.rem(z - block // SLOT + 8, 8)
    hit0 = jnp.where(routes[0:1, :] == expert, 1.0, 0.0)
    hit1 = jnp.where(routes[1:2, :] == expert, 1.0, 0.0)
    member = hit0 + hit1
    before = jnp.where(iota((16, 16), 0) < iota((16, 16), 1), 1.0, 0.0).astype(BF16)
    place = dot(member.astype(BF16), before)
    chosen = jnp.where(place == (block % SLOT).astype(F32), member, 0.0)
    weights = route_w[...].astype(F32)
    scaled = (chosen * (hit0 * weights[0:1, :] + hit1 * weights[1:2, :])).astype(BF16)
    mine = jnp.where(first, chosen[0:32, :], chosen[32:64, :]).astype(BF16)
    pack_s, pack_o, open_s, open_o = pack_matrices(c)

    mix_copy.wait_recv()
    after = (full + (mix_o[...].astype(F32) + mix_p[...].astype(F32))).astype(BF16).astype(F32)
    mean2 = jnp.sum(after * after, axis=1, keepdims=True) / 2048.0
    nf_lo, nf_hi = halves(norm_ffn[...], nf_p[...])
    normed2 = (after * lax.rsqrt(mean2 + epsilon) * jnp.concatenate([nf_lo, nf_hi], axis=1)).astype(BF16)

    rows = dot(mine, normed2)
    for j in range(4):
        disp[SLOT * j : SLOT * (j + 1), :] = rows[SLOT * j : SLOT * (j + 1), :].astype(BF16)
    sent = []
    for j in range(4):
        part = pl.ds(SLOT * j, SLOT)
        sent.append(remote(disp.at[part], zrecv.at[part], shift(Z, -(4 * c + j))))
    for j in (1, 2, 3):
        sent[j].start()

    @pl.when(first)
    def _():
        zrecv[0:SLOT, :] = disp[0:SLOT, :]

    @pl.when(jnp.logical_not(first))
    def _():
        sent[0].start()

    gv_lo, gv_hi = halves(gate_vec[...].astype(F32), gv_p[...].astype(F32))
    logit = jnp.sum(normed2.astype(F32) * jnp.concatenate([gv_lo, gv_hi], axis=1), axis=1, keepdims=True)
    own_rows = dot(pack_o, normed2)

    for j in (1, 2, 3):
        sent[j].wait_recv()

    @pl.when(jnp.logical_not(first))
    def _():
        sent[0].wait_recv()

    packed = (dot(pack_s, zrecv[...]) + own_rows).astype(BF16)
    xs[0, 0:16, :] = packed[0:16, :]
    xs[1, 0:16, :] = packed[16:32, :]

    axes = ((X, Y), (Y, X))

    def cell(ref, half, rq, rp, part=None):
        base = 16 * (4 * rq + rp)
        start, count = (base, 16) if part is None else (base + 8 * part, 8)
        return ref.at[half, pl.ds(start, count)]

    got = [{}, {}]

    def send_p(half, rp):
        q = axes[half][1]
        got[half][1, rp] = started(cell(xs, half, 0, rp), cell(xs, half, 1, rp), shift(q, 1))
        got[half][3, rp] = started(cell(xs, half, 0, rp), cell(xs, half, 3, rp), shift(q, -1))

    def pass_on(half, rp):
        q = axes[half][1]
        if rp in (0, 2):
            got[half][1, rp].wait_recv()
            got[half][2, rp] = started(cell(xs, half, 1, rp), cell(xs, half, 2, rp), shift(q, 1))
        else:
            got[half][3, rp].wait_recv()
            got[half][2, rp] = started(cell(xs, half, 3, rp), cell(xs, half, 2, rp), shift(q, -1))

    for half in range(2):
        p = axes[half][0]
        got[half][0, 1] = started(cell(xs, half, 0, 0), cell(xs, half, 0, 1), shift(p, 1))
        got[half][0, 3] = started(cell(xs, half, 0, 0), cell(xs, half, 0, 3), shift(p, -1))
    for half in range(2):
        send_p(half, 0)
    across = []
    for half in range(2):
        p = axes[half][0]
        got[half][0, 1].wait_recv()
        across.append(started(cell(xs, half, 0, 1, 0), cell(xs, half, 0, 2, 0), shift(p, 1)))
        send_p(half, 1)
        got[half][0, 3].wait_recv()
        across.append(started(cell(xs, half, 0, 3, 1), cell(xs, half, 0, 2, 1), shift(p, -1)))
        send_p(half, 3)
    ring[2].wait_recv()
    ring[3] = started(wd_slot(2), wd_slot(3), shift(Z, 1))
    ring[6].wait_recv()
    ring[5] = started(wd_slot(6), wd_slot(5), shift(Z, -1))
    for half in range(2):
        pass_on(half, 0)
    for half in range(2):
        across[2 * half].wait_recv()
        across[2 * half + 1].wait_recv()
        send_p(half, 2)
    for half in range(2):
        pass_on(half, 1)
    for half in range(2):
        pass_on(half, 3)
    ring[3].wait_recv()
    ring[4] = started(wd_slot(3), wd_slot(4), shift(Z, 1))
    for half in range(2):
        pass_on(half, 2)
    for half in range(2):
        for rp in (1, 3):
            got[half][1, rp].wait_recv()
        for rp in (0, 2):
            got[half][3, rp].wait_recv()
        for rp in range(4):
            got[half][2, rp].wait_recv()

    for copy in loads[5:]:
        copy.wait()
    for copy in swap:
        copy.wait_recv()

    def expert_hidden(half):
        rows = xs[half]
        return silu(dot_nt(rows, we[0])) * dot_nt(rows, we[1])

    def sum_p(ref, half, rq):
        return ref[half, 64 * rq : 64 * (rq + 1), :]

    hidden = expert_hidden(0).astype(BF16)
    for rq in (2, 1, 3, 0):
        for n in range(4):
            outs[0, 64 * rq : 64 * (rq + 1), 512 * n : 512 * (n + 1)] = dot(
                hidden[64 * rq : 64 * (rq + 1), :], we[2, :, 512 * n : 512 * (n + 1)]
            ).astype(BF16)

    got_q = [{}, {}]

    def reduce_opposite(half):
        q = axes[half][1]
        for rp in range(4):
            device = shift(q, -1 if rp in (0, 2) else 1)
            got_q[half][2, rp] = started(cell(outs, half, 2, rp), opp_q.at[half, pl.ds(16 * rp, 16)], device)

    reduce_opposite(0)

    hidden_e = expert_hidden(1)
    ring[5].wait_recv()
    ring[4].wait_recv()
    whole = started(wd.at[:, pl.ds(c, 1)], wd.at[:, pl.ds(c, 1)], partner)
    place_in = iota((256, 1), 0) % 16
    hidden_e = jnp.where(place_in < 4, hidden_e, 0.0).astype(BF16)
    whole.wait_recv()

    def dense_pre(t):
        return dot_nt(xs[1, :, 0:1024], wd[t, 0]) + dot_nt(xs[1, :, 1024:2048], wd[t, 1])

    hidden_d = jnp.where(place_in >= 4, silu(dense_pre(0)) * dense_pre(1), 0.0).astype(BF16)
    for rq in (2, 1, 3, 0):
        take = slice(64 * rq, 64 * (rq + 1))
        for n in range(4):
            outs[1, take, 512 * n : 512 * (n + 1)] = (
                dot(hidden_e[take, :], we[2, :, 512 * n : 512 * (n + 1)])
                + dot(hidden_d[take, :], wd[2, n // 2, :, 512 * (n % 2) : 512 * (n % 2 + 1)])
            ).astype(BF16)
    reduce_opposite(1)

    def reduce_neighbours(half):
        q = axes[half][1]
        for rp in (0, 2, 1, 3):
            rq, by = (1, -1) if rp in (0, 2) else (3, 1)
            got_q[half][2, rp].wait_recv()
            at_row = 16 * (4 * rq + rp)
            both = outs[half, at_row : at_row + 16, :].astype(F32) + opp_q[half, 16 * rp : 16 * rp + 16, :].astype(F32)
            outs[half, at_row : at_row + 16, :] = both.astype(BF16)
        for rp in range(4):
            for rq, by in ((1, -1), (3, 1)):
                got_q[half][rq, rp] = started(
                    cell(outs, half, rq, rp), fin_q.at[half, rq // 2, pl.ds(16 * rp, 16)], shift(q, by)
                )

    got_p = [{}, {}]

    def reduce_p_start(half):
        p = axes[half][0]
        total = []
        for rp in (2, 1, 3, 0):
            for rq in (1, 3):
                got_q[half][rq, rp].wait_recv()
            take = slice(16 * rp, 16 * rp + 16)
            total.append(
                outs[half, take, :].astype(F32) + fin_q[half, 0, take, :].astype(F32) + fin_q[half, 1, take, :].astype(F32)
            )
            if rp == 2:
                tsend[half, take, :] = total[0].astype(BF16)
                got_p[half]["lo"] = started(
                    tsend.at[half, pl.ds(32, 8)], opp_p.at[half, pl.ds(0, 8)], shift(p, -1)
                )
                got_p[half]["hi"] = started(
                    tsend.at[half, pl.ds(40, 8)], opp_p.at[half, pl.ds(8, 8)], shift(p, 1)
                )
        return total

    def reduce_p_next(half, total):
        p = axes[half][0]
        zero = jnp.zeros((8, 2048), F32)
        got_p[half]["lo"].wait_recv()
        extra = jnp.concatenate([opp_p[half, 0:8, :].astype(F32), zero], axis=0)
        tsend[half, 16:32, :] = (total[1] + extra).astype(BF16)
        got_p[half][1] = started(tsend.at[half, pl.ds(16, 16)], fin_p.at[half, 0], shift(p, -1))
        got_p[half]["hi"].wait_recv()
        extra = jnp.concatenate([zero, opp_p[half, 8:16, :].astype(F32)], axis=0)
        tsend[half, 48:64, :] = (total[2] + extra).astype(BF16)
        got_p[half][3] = started(tsend.at[half, pl.ds(48, 16)], fin_p.at[half, 1], shift(p, 1))

    def reduce_end(half, total):
        got_p[half][1].wait_recv()
        got_p[half][3].wait_recv()
        return total[3] + fin_p[half, 0].astype(F32) + fin_p[half, 1].astype(F32)

    reduce_neighbours(0)
    reduce_neighbours(1)
    totals = [reduce_p_start(0), reduce_p_start(1)]
    for half in range(2):
        reduce_p_next(half, totals[half])
    summed = jnp.concatenate([reduce_end(half, totals[half]) for half in range(2)], axis=0).astype(BF16)

    opened = dot(open_s, summed)
    for h in range(2):
        for j in range(4):
            rbuf[h, SLOT * j : SLOT * (j + 1), :] = opened[
                SLOT * j : SLOT * (j + 1), 1024 * h : 1024 * (h + 1)
            ].astype(BF16)

    def ret_copy(j, h, device):
        d = 4 * c + j
        return pltpu.make_async_remote_copy(
            src_ref=rbuf.at[h, pl.ds(SLOT * j, SLOT)],
            dst_ref=ret.at[pl.ds(pl.multiple_of(SLOT * d, SLOT), SLOT)],
            send_sem=ret_send.at[2 * j + h],
            recv_sem=ret_recv.at[d],
            device_id=device,
            device_id_type=MESH,
        )

    def ret_device(j, h):
        return {**shift(Z, 4 * c + j), "tp": h}

    def ret_each(act):
        for j in (1, 2, 3):
            for h in range(2):
                act(ret_copy(j, h, ret_device(j, h)))

        @pl.when(first)
        def _():
            act(ret_copy(0, 1, {"tp": 1}))

        @pl.when(jnp.logical_not(first))
        def _():
            for h in range(2):
                act(ret_copy(0, h, ret_device(0, h)))

    ret_each(lambda copy: copy.start())

    @pl.when(first)
    def _():
        ret[0:SLOT, :] = rbuf[0, 0:SLOT, :]

    dense_rows = dot(open_o, summed)
    own_half, other_half = halves(dense_rows[:, 0:1024], dense_rows[:, 1024:2048])
    dsend[...] = other_half.astype(BF16)
    dense_copy = started(dsend, drecv, partner)
    after_lo, _ = halves(after[:, 0:1024], after[:, 1024:2048])
    dense_copy.wait_recv()
    dense = (own_half + drecv[...].astype(F32)) * (1.0 / (1.0 + jnp.exp(-logit)))

    def ret_wait(d):
        pltpu.make_async_remote_copy(
            src_ref=rbuf.at[0, pl.ds(0, SLOT)],
            dst_ref=ret.at[pl.ds(SLOT * d, SLOT)],
            send_sem=ret_send.at[0],
            recv_sem=ret_recv.at[d],
            device_id=partner,
            device_id_type=MESH,
        ).wait_recv()

    for d in range(1, 8):
        ret_wait(d)

    @pl.when(jnp.logical_not(first))
    def _():
        ret_wait(0)

    moe = dot_tn(scaled, ret[...])
    mixed[...] = (after_lo + moe + dense).astype(BF16)

    keep.wait()
    for copy in pair + swap + across + [mix_copy, whole, dense_copy]:
        copy.wait_send()
    for group in [ring] + got + got_q + got_p:
        for copy in group.values():
            copy.wait_send()
    for j in (1, 2, 3):
        sent[j].wait_send()

    @pl.when(jnp.logical_not(first))
    def _():
        sent[0].wait_send()

    ret_each(lambda copy: copy.wait_send())
    assert used[0] <= COPIES


def body(
    tokens,
    state,
    norm_mix,
    w_query,
    w_key,
    w_value,
    w_out,
    norm_ffn,
    gate_vector,
    dense_gate,
    dense_up,
    dense_down,
    exp_gate,
    exp_up,
    exp_down,
    routes,
    route_w,
):
    vmem = pl.BlockSpec(memory_space=pltpu.VMEM)
    hbm = pl.BlockSpec(memory_space=pl.ANY)

    def buf(*shape, dtype=BF16):
        return pltpu.VMEM(shape, dtype)

    return pl.pallas_call(
        kernel,
        out_shape=(
            jax.ShapeDtypeStruct(tokens.shape, tokens.dtype),
            jax.ShapeDtypeStruct(state.shape, state.dtype),
        ),
        in_specs=[vmem] * 9 + [hbm] * 8,
        out_specs=(vmem, hbm),
        scratch_shapes=[
            buf(2048, 256),
            buf(2048, 256),
            buf(2048, 256),
            buf(256, 2048),
            buf(16, 2, 128, 128, dtype=F32),
            buf(16, 256, dtype=F32),
            buf(16, 1024),
            buf(1, 1024, dtype=F32),
            buf(1, 1024),
            buf(16, 2048),
            buf(16, 2048),
            buf(3, 176, 2048),
            buf(3, 2, 192, 1024),
            buf(32, 2048),
            buf(32, 2048),
            buf(2, 256, 2048),
            buf(2, 256, 2048),
            buf(2, 64, 2048),
            buf(2, 2, 64, 2048),
            buf(2, 64, 2048),
            buf(2, 16, 2048),
            buf(2, 2, 16, 2048),
            buf(2, 32, 1024),
            buf(64, 1024),
            buf(16, 1024),
            buf(16, 1024),
            pltpu.SemaphoreType.DMA((9,)),
            pltpu.SemaphoreType.DMA((COPIES,)),
            pltpu.SemaphoreType.DMA((COPIES,)),
            pltpu.SemaphoreType.DMA((8,)),
            pltpu.SemaphoreType.DMA((8,)),
        ],
        compiler_params=pltpu.CompilerParams(
            collective_id=0, has_side_effects=True, vmem_limit_bytes=48 * 1024 * 1024
        ),
        name="layer",
    )(
        tokens,
        norm_mix.reshape(1, -1),
        norm_ffn.reshape(1, -1),
        gate_vector.reshape(1, -1),
        routes.T,
        route_w.T,
        dense_gate.T,
        dense_up.T,
        dense_down,
        state,
        w_query,
        w_key,
        w_value,
        w_out,
        exp_gate[0].T,
        exp_up[0].T,
        exp_down[0],
    )


def solution(mesh):
    finer = Mesh(mesh.devices.reshape(8, 4, 4, mesh.shape["tp"]), (*EP, "tp"))
    in_specs = (
        P(EP, "tp"),
        P(EP, "tp", None, None),
        P(),
        P(None, "tp"),
        P(None, "tp"),
        P(None, "tp"),
        P("tp", None),
        P("tp"),
        P("tp"),
        P("tp", EP),
        P("tp", EP),
        P(EP, "tp"),
        P(EP, None, "tp"),
        P(EP, None, "tp"),
        P(EP, "tp", None),
        P(EP, None),
        P(EP, None),
    )
    out_specs = (P(EP, "tp"), P(EP, "tp", None, None))
    return jax.shard_map(body, mesh=finer, in_specs=in_specs, out_specs=out_specs, check_vma=False)
```

```python
import jax
import jax.numpy as jnp
from jax import lax
from jax.experimental import pallas as pl
from jax.experimental.pallas import tpu as pltpu
from jax.sharding import Mesh
from jax.sharding import PartitionSpec as P

EP = ("ep_0", "ep_1", "ep_2")
Z, Y, X = EP
MESH = pl.DeviceIdType.MESH
SLOT = 8
CAP = 5
F32 = jnp.float32
BF16 = jnp.bfloat16
epsilon = 1e-06
COPIES = 80
AT = {2: 0, 1: 1, 3: 2, 0: 3}
PASS = {0: -1, 1: 1, 3: -1}


def iota(shape, dim):
    return lax.broadcasted_iota(jnp.int32, shape, dim)


def dot(a, b):
    return jnp.dot(a, b, preferred_element_type=F32)


def dot_nt(a, b):
    return lax.dot_general(a, b, (((1,), (1,)), ((), ())), preferred_element_type=F32)


def dot_tn(a, b):
    return lax.dot_general(a, b, (((0,), (0,)), ((), ())), preferred_element_type=F32)


def silu(v):
    return v / (1.0 + jnp.exp(-v))


def pack_matrix(row, col):
    return jnp.where((row < 4 * CAP) & (col == row // CAP * SLOT + row % CAP), 1.0, 0.0).astype(BF16)


def kernel(
    tokens_h,
    norm_mix_h,
    norm_ffn_h,
    gate_vec_h,
    routes_h,
    route_w_h,
    dgate_h,
    dup_h,
    ddown_h,
    state,
    w_query,
    w_key,
    w_value,
    w_out,
    egate,
    eup,
    edown,
    mixed,
    key_out,
    value_out,
    tokens,
    norm_mix,
    norm_ffn,
    gate_vec,
    routes,
    route_w,
    dgate,
    dup,
    ddown,
    wq,
    wk,
    wv,
    wo,
    st,
    read,
    tok_p,
    nf_p,
    mix_o,
    mix_p,
    we,
    wd,
    disp,
    zrecv,
    xs,
    outs,
    opp_q,
    fin_q,
    tsend,
    fin_p,
    rbuf,
    ret,
    local_sem,
    send_sem,
    recv_sem,
    ret_send,
    ret_recv,
):
    z, y, x, c = (lax.axis_index(a) for a in (Z, Y, X, "tp"))
    first = c == 0
    used = [0]

    def wrap(value, size):
        return lax.rem(value + size, size)

    def along_z(by):
        return {Z: wrap(z + by, 8)}

    def along_p(by):
        return {X: wrap(x + by * (1 - c), 4), Y: wrap(y + by * c, 4)}

    def along_q(by):
        return {X: wrap(x + by * c, 4), Y: wrap(y + by * (1 - c), 4)}

    partner = {"tp": 1 - c}

    def remote(src, dst, device):
        n = used[0]
        used[0] += 1
        return pltpu.make_async_remote_copy(
            src_ref=src,
            dst_ref=dst,
            send_sem=send_sem.at[n],
            recv_sem=recv_sem.at[n],
            device_id=device,
            device_id_type=MESH,
        )

    sent = []

    def started(src, dst, device):
        copy = remote(src, dst, device)
        copy.start()
        sent.append(copy)
        return copy

    def halves(own, other):
        return jnp.where(first, own, other), jnp.where(first, other, own)

    def as_row(ref):
        rows = ref[...].astype(F32)
        return jnp.concatenate([rows[i : i + 1, :] for i in range(8)], axis=1)

    loads = {}
    for n, (src, dst) in enumerate(
        [
            (tokens_h, tokens),
            (norm_ffn_h, norm_ffn),
            (dgate_h, dgate),
            (dup_h, dup),
            (ddown_h, ddown),
            (gate_vec_h, gate_vec),
            (norm_mix_h, norm_mix),
            (routes_h, routes),
            (route_w_h, route_w),
            (w_query, wq),
            (w_key, wk),
            (w_value, wv),
            (state, st),
            (w_out, wo),
            (egate, we.at[0, pl.ds(0, 88)]),
            (eup, we.at[1, pl.ds(0, 88)]),
            (edown, we.at[2, pl.ds(0, 88)]),
        ]
    ):
        loads[n] = pltpu.make_async_copy(src, dst, local_sem.at[n])
        loads[n].start()

    barrier = pltpu.get_barrier_semaphore()
    peers = [partner]
    for by in range(1, 8):
        for core in (c, 1 - c):
            peers.append({**along_z(by), "tp": core})
    for by in (1, -1, 2):
        peers += [along_p(by), along_q(by)]
    for peer in peers:
        pl.semaphore_signal(barrier, inc=1, device_id=peer, device_id_type=MESH)

    for n in range(9):
        loads[n].wait()
    tail = jnp.zeros((2, 1024), F32)
    gate_tail = jnp.concatenate([as_row(gate_vec), tail[0:1, :]], axis=0)
    for t, (ref, end) in enumerate(((dgate, gate_tail), (dup, tail), (ddown, tail))):
        block = jnp.concatenate([ref[...].astype(F32), end], axis=0)
        wd[t, pl.ds(c, 1), pl.ds(0, 24), :] = block.astype(BF16)[None]

    pl.semaphore_wait(barrier, len(peers))

    pair = [started(tokens, tok_p, partner), started(norm_ffn, nf_p, partner)]

    def wd_slot(n):
        return wd.at[:, pl.ds(c, 1), pl.ds(24 * n, 24), :]

    ring, cross = {}, {}

    def forward(source, target):
        ring[target] = started(wd_slot(source), wd_slot(target), along_z(1 if target < 5 else -1))

    def last(source, start, count, by):
        def part(n):
            return wd.at[pl.ds(start, count), pl.ds(c, 1), pl.ds(24 * n, 24), :]

        ring[4, by] = started(part(source), part(4), along_z(by))

    def across(n):
        cross[n] = started(wd_slot(n), wd_slot(n), partner)

    forward(0, 1)
    forward(0, 7)
    swap = [started(src, we.at[t, pl.ds(88, 88)], partner) for t, src in enumerate((egate, eup, edown))]
    across(0)

    for copy in pair:
        copy.wait_recv()
    lo, hi = halves(tokens[...].astype(F32), tok_p[...].astype(F32))
    full = jnp.concatenate([lo, hi], axis=1)
    mean = jnp.sum(full * full, axis=1, keepdims=True) / 2048.0
    normed = (full * lax.rsqrt(mean + epsilon) * norm_mix[...]).astype(BF16)
    for n in (9, 10, 11):
        loads[n].wait()
    query = dot(normed, wq[...]).astype(BF16).astype(F32)
    key = dot(normed, wk[...]).astype(BF16).astype(F32) * 128 ** (-0.5)
    value = dot(normed, wv[...]).astype(BF16).astype(F32)
    key_out[...] = key
    value_out[...] = value
    blank = jnp.zeros((112, 256), F32)
    query_t = jnp.concatenate([query, blank], axis=0).T
    key_t = jnp.concatenate([key, blank], axis=0).T
    loads[12].wait()
    for h in range(2):
        decay = jnp.where(first, 1.0 - 2.0 ** (-3.0 - 2.0 * h), 1.0 - 2.0 ** (-7.0 - 2.0 * h))
        for s in range(16):
            k_col = key_t[h * 128 : (h + 1) * 128, s : s + 1]
            q_col = query_t[h * 128 : (h + 1) * 128, s : s + 1]
            v_row = value[s : s + 1, h * 128 : (h + 1) * 128]
            new = decay * st[s, h] + k_col * v_row
            read[s : s + 1, h * 128 : (h + 1) * 128] = jnp.sum(q_col * new, axis=0, keepdims=True)
    heads = []
    for h in range(2):
        part = read[:, h * 128 : (h + 1) * 128]
        centre = jnp.mean(part, axis=1, keepdims=True)
        spread = jnp.mean(jnp.square(part - centre), axis=1, keepdims=True)
        heads.append(((part - centre) * lax.rsqrt(spread + epsilon)).astype(BF16))
    loads[13].wait()
    mix = dot(heads[0], wo[0:128, :]) + dot(heads[1], wo[128:256, :])
    mix_o[...] = mix.astype(BF16)
    mix_copy = started(mix_o, mix_p, partner)

    block = iota((64, 16), 0)
    expert = lax.rem(z - block // SLOT + 8, 8)
    hit0 = jnp.where(routes[0:1, :] == expert, 1.0, 0.0)
    hit1 = jnp.where(routes[1:2, :] == expert, 1.0, 0.0)
    member = hit0 + hit1
    before = jnp.where(iota((16, 16), 0) < iota((16, 16), 1), 1.0, 0.0).astype(BF16)
    place = dot(member.astype(BF16), before)
    chosen = jnp.where(place == (block % SLOT).astype(F32), member, 0.0)
    weights = route_w[...].astype(F32)
    slot_w = jnp.sum(chosen * (hit0 * weights[0:1, :] + hit1 * weights[1:2, :]), axis=1, keepdims=True)
    slot_first = jnp.sum(chosen * hit0, axis=1, keepdims=True)
    lane = iota((64, 128), 1)
    extra = jnp.where(lane == 0, slot_w, jnp.where(lane == 1, slot_first, 0.0))
    extra = jnp.where(first, extra[0:32, :], extra[32:64, :]).astype(BF16)
    mine = jnp.where(first, chosen[0:32, :], chosen[32:64, :]).astype(BF16)

    mix_copy.wait_recv()
    after = (full + (mix_o[...].astype(F32) + mix_p[...].astype(F32))).astype(BF16).astype(F32)
    mean2 = jnp.sum(after * after, axis=1, keepdims=True) / 2048.0
    nf_lo, nf_hi = halves(norm_ffn[...], nf_p[...])
    normed2 = (after * lax.rsqrt(mean2 + epsilon) * jnp.concatenate([nf_lo, nf_hi], axis=1)).astype(BF16)

    rows = dot(mine, normed2)
    disp[:, 2048:2176] = extra
    disp[:, 0:2048] = rows.astype(BF16)
    moved = []
    for j in range(4):
        part = pl.ds(SLOT * j, SLOT)
        moved.append(remote(disp.at[part], zrecv.at[part], along_z(-(4 * c + j))))
    for j in (3, 2, 1):
        moved[j].start()

    @pl.when(first)
    def _():
        zrecv[0:SLOT, :] = disp[0:SLOT, :]

    @pl.when(jnp.logical_not(first))
    def _():
        moved[0].start()

    ring[1].wait_recv()
    forward(1, 2)
    ring[7].wait_recv()
    forward(7, 6)
    across(1)
    across(7)

    for j in (1, 2, 3):
        moved[j].wait_recv()

    @pl.when(jnp.logical_not(first))
    def _():
        moved[0].wait_recv()

    def cell(ref, rq, rp, start=0, count=24):
        return ref.at[pl.ds(24 * (4 * AT[rq] + rp) + start, count)]

    def cell_rows(ref, rq, rp):
        base = 24 * (4 * AT[rq] + rp)
        return ref[base : base + 24, :].astype(F32)

    def set_rows(ref, rq, rp, rows):
        base = 24 * (4 * AT[rq] + rp)
        ref[base : base + 24, :] = rows.astype(BF16)

    set_rows(xs, 0, 0, dot(pack_matrix(iota((24, 32), 0), iota((24, 32), 1)), zrecv[...]))

    got = {}

    def send_q(rp):
        got[1, rp] = started(cell(xs, 0, rp), cell(xs, 1, rp), along_q(1))
        got[3, rp] = started(cell(xs, 0, rp), cell(xs, 3, rp), along_q(-1))

    def pass_on(rp):
        by = PASS[rp]
        near = 2 - by
        got[near, rp].wait_recv()
        got[2, rp] = started(cell(xs, near, rp), cell(xs, 2, rp), along_q(by))

    got[0, 1] = started(cell(xs, 0, 0), cell(xs, 0, 1), along_p(1))
    got[0, 3] = started(cell(xs, 0, 0), cell(xs, 0, 3), along_p(-1))
    got[0, 2] = started(cell(xs, 0, 0), cell(xs, 0, 2), along_p(2))
    send_q(0)
    got[0, 1].wait_recv()
    send_q(1)
    got[0, 3].wait_recv()
    send_q(3)
    pass_on(0)
    ring[2].wait_recv()
    forward(2, 3)
    ring[6].wait_recv()
    forward(6, 5)
    across(2)
    across(6)
    got[0, 2].wait_recv()
    send_q(2)
    got[2, 2] = started(cell(xs, 0, 2), cell(xs, 2, 2), along_q(2))
    pass_on(1)
    pass_on(3)
    ring[3].wait_recv()
    last(3, 0, 2, 1)
    across(3)
    ring[5].wait_recv()
    last(5, 2, 1, -1)
    across(5)
    for rp in range(4):
        for rq in (1, 3):
            if rp == 2 or PASS[rp] != 2 - rq:
                got[rq, rp].wait_recv()

    for n in (14, 15, 16):
        loads[n].wait()
    for copy in swap:
        copy.wait_recv()

    def hidden_rows(start, count):
        rows = xs[start : start + count, 0:2048]
        scale = xs[start : start + count, 2048:2049].astype(F32)
        return (silu(dot_nt(rows, we[0])) * dot_nt(rows, we[1]) * scale).astype(BF16)

    hidden_near = hidden_rows(96, 288)
    for rp in range(4):
        got[2, rp].wait_recv()
    hidden_far = hidden_rows(0, 96)

    ring[4, 1].wait_recv()
    ring[4, -1].wait_recv()
    across(4)
    for n in range(8):
        cross[n].wait_recv()

    def dense_pre(t):
        return dot_nt(xs[:, 0:1024], wd[t, 0]) + dot_nt(xs[:, 1024:2048], wd[t, 1])

    pre = dense_pre(0)
    dense_scale = xs[:, 2049:2050].astype(F32) / (1.0 + jnp.exp(-pre[:, 22:23]))
    hidden_d = (silu(pre) * dense_pre(1) * dense_scale).astype(BF16)

    def down(hidden_e, start, count):
        take = slice(start, start + count)
        for n in range(4):
            outs[take, 512 * n : 512 * (n + 1)] = (
                dot(hidden_e, we[2, :, 512 * n : 512 * (n + 1)])
                + dot(hidden_d[take, :], wd[2, n // 2, :, 512 * (n % 2) : 512 * (n % 2 + 1)])
            ).astype(BF16)

    back = {}

    def at_rp(ref, rp):
        return ref.at[pl.ds(24 * rp, 24)]

    def rp_rows(ref, rp):
        return ref[24 * rp : 24 * rp + 24, :].astype(F32)

    down(hidden_far, 0, 96)
    direct = started(cell(outs, 2, 2), at_rp(opp_q, 2), along_q(2))
    for rp in (1, 3, 0):
        back[2, rp] = started(cell(outs, 2, rp), at_rp(opp_q, rp), along_q(-PASS[rp]))
    down(hidden_near, 96, 288)

    def send_back(rq, rp):
        back[rq, rp] = started(cell(outs, rq, rp), at_rp(fin_q.at[rq // 2], rp), along_q(-1 if rq == 1 else 1))

    for rq, rp in ((1, 2), (3, 2), (1, 1), (3, 1), (1, 3), (3, 3), (1, 0), (3, 0)):
        if rp == 2 or PASS[rp] != 2 - rq:
            send_back(rq, rp)
    for rp in (1, 3, 0):
        rq = 2 - PASS[rp]
        back[2, rp].wait_recv()
        set_rows(outs, rq, rp, cell_rows(outs, rq, rp) + rp_rows(opp_q, rp))
        send_back(rq, rp)

    total = {}

    def sum_q(rp):
        for rq in (1, 3):
            back[rq, rp].wait_recv()
        total[rp] = cell_rows(outs, 0, rp) + rp_rows(fin_q.at[0], rp) + rp_rows(fin_q.at[1], rp)

    def send_p(n, rp, by):
        rows = pl.ds(24 * n, 24)
        tsend[24 * n : 24 * n + 24, :] = total[rp].astype(BF16)
        back["p", n] = started(tsend.at[rows], fin_p.at[rows], along_p(by))

    sum_q(2)
    direct.wait_recv()
    total[2] = total[2] + rp_rows(opp_q, 2)
    send_p(0, 2, 2)
    sum_q(1)
    send_p(1, 1, -1)
    sum_q(3)
    send_p(2, 3, 1)
    sum_q(0)
    for n in range(3):
        back["p", n].wait_recv()
    summed = (total[0] + rp_rows(fin_p, 0) + rp_rows(fin_p, 1) + rp_rows(fin_p, 2)).astype(BF16)

    opened = dot(pack_matrix(iota((32, 24), 1), iota((32, 24), 0)), summed)
    for h in range(2):
        rbuf[h] = opened[:, 1024 * h : 1024 * (h + 1)].astype(BF16)

    def ret_copy(j, h, device):
        d = 4 * c + j
        return pltpu.make_async_remote_copy(
            src_ref=rbuf.at[h, pl.ds(SLOT * j, SLOT)],
            dst_ref=ret.at[pl.ds(pl.multiple_of(SLOT * d, SLOT), SLOT)],
            send_sem=ret_send.at[2 * j + h],
            recv_sem=ret_recv.at[d],
            device_id=device,
            device_id_type=MESH,
        )

    def ret_device(j, h):
        return {**along_z(4 * c + j), "tp": h}

    def ret_each(act):
        for j in (3, 2, 1):
            for h in range(2):
                act(ret_copy(j, h, ret_device(j, h)))

        @pl.when(first)
        def _():
            act(ret_copy(0, 1, {"tp": 1}))

        @pl.when(jnp.logical_not(first))
        def _():
            for h in range(2):
                act(ret_copy(0, h, ret_device(0, h)))

    ret_each(lambda copy: copy.start())

    @pl.when(first)
    def _():
        ret[0:SLOT, :] = rbuf[0, 0:SLOT, :]

    def ret_wait(d):
        pltpu.make_async_remote_copy(
            src_ref=rbuf.at[0, pl.ds(0, SLOT)],
            dst_ref=ret.at[pl.ds(SLOT * d, SLOT)],
            send_sem=ret_send.at[0],
            recv_sem=ret_recv.at[d],
            device_id=partner,
            device_id_type=MESH,
        ).wait_recv()

    after_own, _ = halves(after[:, 0:1024], after[:, 1024:2048])
    for d in range(1, 8):
        ret_wait(d)

    @pl.when(jnp.logical_not(first))
    def _():
        ret_wait(0)

    mixed[...] = after_own + dot_tn(chosen.astype(BF16), ret[...])

    for copy in sent:
        copy.wait_send()
    for j in (1, 2, 3):
        moved[j].wait_send()

    @pl.when(jnp.logical_not(first))
    def _():
        moved[0].wait_send()

    ret_each(lambda copy: copy.wait_send())
    assert used[0] <= COPIES


def finish(summed_h, key_h, value_h, state_h, mixed_h, new_h, summed, key, value, mixed, st, sem, in_sem, out_sem):
    small = [
        pltpu.make_async_copy(src, dst, sem.at[n])
        for n, (src, dst) in enumerate(((key_h, key), (value_h, value), (summed_h, summed)))
    ]
    for copy in small:
        copy.start()
    pieces = []
    for n in range(8):
        part = pl.ds(2 * n, 2)
        pieces.append(pltpu.make_async_copy(state_h.at[part], st.at[part], in_sem.at[n]))
        pieces[n].start()
    for copy in small:
        copy.wait()
    mixed[...] = summed[...].astype(BF16)
    stores = [pltpu.make_async_copy(mixed, mixed_h, out_sem.at[8])]
    stores[0].start()
    key_t = jnp.concatenate([key[...], jnp.zeros((112, 256), F32)], axis=0).T
    first = lax.axis_index("tp") == 0
    decay = [jnp.where(first, 1.0 - 2.0 ** (-3.0 - 2.0 * h), 1.0 - 2.0 ** (-7.0 - 2.0 * h)) for h in range(2)]
    for n in range(8):
        pieces[n].wait()
        for s in (2 * n, 2 * n + 1):
            for h in range(2):
                span = slice(128 * h, 128 * h + 128)
                st[s, h] = decay[h] * st[s, h] + key_t[span, s : s + 1] * value[s : s + 1, span]
        part = pl.ds(2 * n, 2)
        stores.append(pltpu.make_async_copy(st.at[part], new_h.at[part], out_sem.at[n]))
        stores[-1].start()
    for copy in stores:
        copy.wait()


def body(
    tokens,
    state,
    norm_mix,
    w_query,
    w_key,
    w_value,
    w_out,
    norm_ffn,
    gate_vector,
    dense_gate,
    dense_up,
    dense_down,
    exp_gate,
    exp_up,
    exp_down,
    routes,
    route_w,
):
    vmem = pl.BlockSpec(memory_space=pltpu.VMEM)
    hbm = pl.BlockSpec(memory_space=pltpu.HBM)

    def buf(*shape, dtype=BF16):
        return pltpu.VMEM(shape, dtype)

    summed, key, value = pl.pallas_call(
        kernel,
        out_shape=(
            jax.ShapeDtypeStruct(tokens.shape, F32),
            jax.ShapeDtypeStruct((16, 256), F32),
            jax.ShapeDtypeStruct((16, 256), F32),
        ),
        in_specs=[hbm] * 17,
        out_specs=(vmem, vmem, vmem),
        scratch_shapes=[
            buf(16, 1024),
            buf(1, 2048, dtype=F32),
            buf(1, 1024, dtype=F32),
            buf(8, 128),
            buf(2, 16, dtype=jnp.int32),
            buf(2, 16),
            buf(22, 1024),
            buf(22, 1024),
            buf(22, 1024),
            buf(2048, 256),
            buf(2048, 256),
            buf(2048, 256),
            buf(256, 2048),
            buf(16, 2, 128, 128, dtype=F32),
            buf(16, 256, dtype=F32),
            buf(16, 1024),
            buf(1, 1024, dtype=F32),
            buf(16, 2048),
            buf(16, 2048),
            buf(3, 176, 2048),
            buf(3, 2, 192, 1024),
            buf(32, 2176),
            buf(32, 2176),
            buf(384, 2176),
            buf(384, 2048),
            buf(96, 2048),
            buf(2, 96, 2048),
            buf(72, 2048),
            buf(72, 2048),
            buf(2, 32, 1024),
            buf(64, 1024),
            pltpu.SemaphoreType.DMA((17,)),
            pltpu.SemaphoreType.DMA((COPIES,)),
            pltpu.SemaphoreType.DMA((COPIES,)),
            pltpu.SemaphoreType.DMA((8,)),
            pltpu.SemaphoreType.DMA((8,)),
        ],
        compiler_params=pltpu.CompilerParams(collective_id=0, has_side_effects=True, vmem_limit_bytes=67043328),
        name="layer",
    )(
        tokens,
        norm_mix.reshape(1, -1),
        norm_ffn.reshape(1, -1),
        gate_vector.reshape(8, 128),
        routes.T,
        route_w.T,
        dense_gate.T,
        dense_up.T,
        dense_down,
        state,
        w_query,
        w_key,
        w_value,
        w_out,
        exp_gate[0].T,
        exp_up[0].T,
        exp_down[0],
    )
    return pl.pallas_call(
        finish,
        out_shape=(
            jax.ShapeDtypeStruct(tokens.shape, tokens.dtype),
            jax.ShapeDtypeStruct(state.shape, state.dtype),
        ),
        in_specs=[hbm] * 4,
        out_specs=(hbm, hbm),
        scratch_shapes=[
            buf(16, 1024, dtype=F32),
            buf(16, 256, dtype=F32),
            buf(16, 256, dtype=F32),
            buf(16, 1024),
            buf(16, 2, 128, 128, dtype=F32),
            pltpu.SemaphoreType.DMA((3,)),
            pltpu.SemaphoreType.DMA((8,)),
            pltpu.SemaphoreType.DMA((9,)),
        ],
        compiler_params=pltpu.CompilerParams(vmem_limit_bytes=67043328),
        name="finish",
    )(summed, key, value, state)


def solution(mesh):
    finer = Mesh(mesh.devices.reshape(8, 4, 4, mesh.shape["tp"]), (*EP, "tp"))
    in_specs = (
        P(EP, "tp"),
        P(EP, "tp", None, None),
        P(),
        P(None, "tp"),
        P(None, "tp"),
        P(None, "tp"),
        P("tp", None),
        P("tp"),
        P("tp"),
        P("tp", EP),
        P("tp", EP),
        P(EP, "tp"),
        P(EP, None, "tp"),
        P(EP, None, "tp"),
        P(EP, "tp", None),
        P(EP, None),
        P(EP, None),
    )
    out_specs = (P(EP, "tp"), P(EP, "tp", None, None))
    return jax.shard_map(body, mesh=finer, in_specs=in_specs, out_specs=out_specs, check_vma=False)
```

```python
import jax
import jax.numpy as jnp
from jax import lax
from jax.experimental import pallas as pl
from jax.experimental.pallas import tpu as pltpu
from jax.sharding import Mesh
from jax.sharding import PartitionSpec as P

EP = ("ep_0", "ep_1", "ep_2")
Z, Y, X = EP
MESH = pl.DeviceIdType.MESH
SLOT = 8
CAP = 5
F32 = jnp.float32
BF16 = jnp.bfloat16
epsilon = 1e-06
COPIES = 80
AT = {2: 0, 1: 1, 3: 2, 0: 3}
PASS = {0: -1, 1: 1, 3: -1}


def iota(shape, dim):
    return lax.broadcasted_iota(jnp.int32, shape, dim)


def dot(a, b):
    return jnp.dot(a, b, preferred_element_type=F32)


def dot_nt(a, b):
    return lax.dot_general(a, b, (((1,), (1,)), ((), ())), preferred_element_type=F32)


def dot_tn(a, b):
    return lax.dot_general(a, b, (((0,), (0,)), ((), ())), preferred_element_type=F32)


def silu(v):
    return v / (1.0 + jnp.exp(-v))


def pack_matrix(row, col, half):
    main = row < 32
    slot = jnp.where(main, row % 16, 16 + row % 4)
    part = jnp.where(main, row // 16, (row - 32) // 4)
    return jnp.where((part == half) & (col == slot // CAP * SLOT + slot % CAP), 1.0, 0.0).astype(BF16)


def kernel(
    tokens_h,
    norm_mix_h,
    norm_ffn_h,
    gate_vec_h,
    routes_h,
    route_w_h,
    dgate_h,
    dup_h,
    ddown_h,
    state,
    w_query,
    w_key,
    w_value,
    w_out,
    egate,
    eup,
    edown,
    mixed,
    st,
    tokens,
    norm_mix,
    norm_ffn,
    gate_vec,
    routes,
    route_w,
    dgate,
    dup,
    ddown,
    wq,
    wk,
    wv,
    wo,
    read,
    tok_p,
    nf_p,
    mix_o,
    mix_p,
    we,
    wd,
    disp,
    zrecv,
    xs,
    sc,
    outs,
    opp_q,
    fin_q,
    tsend,
    fin_p,
    rbuf,
    ret,
    local_sem,
    send_sem,
    recv_sem,
    ret_send,
    ret_recv,
):
    z, y, x, c = (lax.axis_index(a) for a in (Z, Y, X, "tp"))
    first = c == 0
    used = [0]

    def wrap(value, size):
        return lax.rem(value + size, size)

    def along_z(by):
        return {Z: wrap(z + by, 8)}

    def along_p(by):
        return {X: wrap(x + by * (1 - c), 4), Y: wrap(y + by * c, 4)}

    def along_q(by):
        return {X: wrap(x + by * c, 4), Y: wrap(y + by * (1 - c), 4)}

    partner = {"tp": 1 - c}

    def remote(src, dst, device):
        n = used[0]
        used[0] += 1
        return pltpu.make_async_remote_copy(
            src_ref=src,
            dst_ref=dst,
            send_sem=send_sem.at[n],
            recv_sem=recv_sem.at[n],
            device_id=device,
            device_id_type=MESH,
        )

    sent = []

    def started(src, dst, device):
        copy = remote(src, dst, device)
        copy.start()
        sent.append(copy)
        return copy

    def halves(own, other):
        return jnp.where(first, own, other), jnp.where(first, other, own)

    def as_row(ref):
        rows = ref[...].astype(F32)
        return jnp.concatenate([rows[i : i + 1, :] for i in range(8)], axis=1)

    loads = {}
    for n, (src, dst) in enumerate(
        [
            (tokens_h, tokens),
            (norm_ffn_h, norm_ffn),
            (dgate_h, dgate),
            (dup_h, dup),
            (ddown_h, ddown),
            (gate_vec_h, gate_vec),
            (norm_mix_h, norm_mix),
            (routes_h, routes),
            (route_w_h, route_w),
            (w_query, wq),
            (w_key, wk),
            (w_value, wv),
            (state, st),
            (w_out, wo),
            (egate, we.at[0, pl.ds(0, 88)]),
            (eup, we.at[1, pl.ds(0, 88)]),
            (edown, we.at[2, pl.ds(0, 88)]),
        ]
    ):
        loads[n] = pltpu.make_async_copy(src, dst, local_sem.at[n])
        loads[n].start()

    barrier = pltpu.get_barrier_semaphore()
    peers = [partner]
    for by in range(1, 8):
        for core in (c, 1 - c):
            peers.append({**along_z(by), "tp": core})
    for by in (1, -1, 2):
        peers += [along_p(by), along_q(by)]
    for peer in peers:
        pl.semaphore_signal(barrier, inc=1, device_id=peer, device_id_type=MESH)

    for n in range(9):
        loads[n].wait()
    tail = jnp.zeros((2, 1024), F32)
    gate_tail = jnp.concatenate([as_row(gate_vec), tail[0:1, :]], axis=0)
    for t, (ref, end) in enumerate(((dgate, gate_tail), (dup, tail), (ddown, tail))):
        block = jnp.concatenate([ref[...].astype(F32), end], axis=0)
        wd[t, pl.ds(c, 1), pl.ds(0, 24), :] = block.astype(BF16)[None]

    pl.semaphore_wait(barrier, len(peers))

    pair = [started(tokens, tok_p, partner), started(norm_ffn, nf_p, partner)]

    def wd_slot(n):
        return wd.at[:, pl.ds(c, 1), pl.ds(24 * (n - (n > 4)), 24), :]

    ring, cross = {}, {}

    def forward(source, target):
        ring[target] = started(wd_slot(source), wd_slot(target), along_z(1 if target < 4 else -1))

    def across(n):
        cross[n] = started(wd_slot(n), wd_slot(n), partner)

    forward(0, 1)
    forward(0, 7)
    swap = [started(src, we.at[t, pl.ds(88, 88)], partner) for t, src in enumerate((egate, eup, edown))]
    across(0)

    for copy in pair:
        copy.wait_recv()
    lo, hi = halves(tokens[...].astype(F32), tok_p[...].astype(F32))
    full = jnp.concatenate([lo, hi], axis=1)
    mean = jnp.sum(full * full, axis=1, keepdims=True) / 2048.0
    normed = (full * lax.rsqrt(mean + epsilon) * norm_mix[...]).astype(BF16)
    for n in (9, 10, 11):
        loads[n].wait()
    query = dot(normed, wq[...]).astype(BF16).astype(F32)
    key = dot(normed, wk[...]).astype(BF16).astype(F32) * 128 ** (-0.5)
    value = dot(normed, wv[...]).astype(BF16).astype(F32)
    blank = jnp.zeros((112, 256), F32)
    query_t = jnp.concatenate([query, blank], axis=0).T
    key_t = jnp.concatenate([key, blank], axis=0).T
    loads[12].wait()
    for h in range(2):
        decay = jnp.where(first, 1.0 - 2.0 ** (-3.0 - 2.0 * h), 1.0 - 2.0 ** (-7.0 - 2.0 * h))
        for s in range(16):
            k_col = key_t[h * 128 : (h + 1) * 128, s : s + 1]
            q_col = query_t[h * 128 : (h + 1) * 128, s : s + 1]
            v_row = value[s : s + 1, h * 128 : (h + 1) * 128]
            new = decay * st[s, h] + k_col * v_row
            st[s, h] = new
            read[s : s + 1, h * 128 : (h + 1) * 128] = jnp.sum(q_col * new, axis=0, keepdims=True)
    heads = []
    for h in range(2):
        part = read[:, h * 128 : (h + 1) * 128]
        centre = jnp.mean(part, axis=1, keepdims=True)
        spread = jnp.mean(jnp.square(part - centre), axis=1, keepdims=True)
        heads.append(((part - centre) * lax.rsqrt(spread + epsilon)).astype(BF16))
    loads[13].wait()
    mix = dot(heads[0], wo[0:128, :]) + dot(heads[1], wo[128:256, :])
    mix_o[...] = mix.astype(BF16)
    mix_copy = started(mix_o, mix_p, partner)

    block = iota((64, 16), 0)
    expert = lax.rem(z - block // SLOT + 8, 8)
    hit0 = jnp.where(routes[0:1, :] == expert, 1.0, 0.0)
    hit1 = jnp.where(routes[1:2, :] == expert, 1.0, 0.0)
    member = hit0 + hit1
    before = jnp.where(iota((16, 16), 0) < iota((16, 16), 1), 1.0, 0.0).astype(BF16)
    place = dot(member.astype(BF16), before)
    chosen = jnp.where(place == (block % SLOT).astype(F32), member, 0.0)
    weights = route_w[...].astype(F32)
    slot_w = jnp.sum(chosen * (hit0 * weights[0:1, :] + hit1 * weights[1:2, :]), axis=1, keepdims=True)
    other = jnp.where(hit0 > 0.0, routes[1:2, :], routes[0:1, :])
    absent = lax.rem(expert - other + 12, 8)
    absent = jnp.where(absent > 4, absent - 1, absent).astype(F32)
    slot_absent = jnp.sum(chosen * absent, axis=1, keepdims=True)
    extra = jnp.where(iota((64, 128), 1) % 2 == 0, slot_w, slot_absent)
    extra = jnp.where(first, extra[0:32, :], extra[32:64, :]).astype(BF16)
    mine = jnp.where(first, chosen[0:32, :], chosen[32:64, :]).astype(BF16)

    mix_copy.wait_recv()
    after = (full + (mix_o[...].astype(F32) + mix_p[...].astype(F32))).astype(BF16).astype(F32)
    mean2 = jnp.sum(after * after, axis=1, keepdims=True) / 2048.0
    nf_lo, nf_hi = halves(norm_ffn[...], nf_p[...])
    normed2 = (after * lax.rsqrt(mean2 + epsilon) * jnp.concatenate([nf_lo, nf_hi], axis=1)).astype(BF16)

    rows = dot(mine, normed2)
    disp[:, 2048:2176] = extra
    disp[:, 0:2048] = rows.astype(BF16)
    moved = []
    for j in range(4):
        part = pl.ds(SLOT * j, SLOT)
        moved.append(remote(disp.at[part], zrecv.at[part], along_z(-(4 * c + j))))

    @pl.when(first)
    def _():
        for j in (3, 2, 1):
            moved[j].start()
        zrecv[0:SLOT, :] = disp[0:SLOT, :]

    @pl.when(jnp.logical_not(first))
    def _():
        for j in range(4):
            moved[j].start()

    ring[1].wait_recv()
    forward(1, 2)
    ring[7].wait_recv()
    forward(7, 6)
    across(1)
    across(7)

    for j in (1, 2, 3):
        moved[j].wait_recv()

    @pl.when(jnp.logical_not(first))
    def _():
        moved[0].wait_recv()

    def cell(ref, rq, rp):
        return ref.at[4 * AT[rq] + rp]

    def cell_rows(ref, rq, rp):
        return ref[4 * AT[rq] + rp].astype(F32)

    def set_rows(ref, rq, rp, rows):
        ref[4 * AT[rq] + rp] = rows.astype(BF16)

    row, col = iota((40, 32), 0), iota((40, 32), 1)
    packed = dot(pack_matrix(row, col, 0), zrecv[:, 0:1024]) + dot(pack_matrix(row, col, 1), zrecv[:, 1024:2048])
    set_rows(xs, 0, 0, packed)
    lane8, row8, col8 = iota((8, 128), 1), iota((8, 32), 0), iota((8, 32), 1)

    def scalars(slot):
        pick = jnp.where(col8 == slot // CAP * SLOT + slot % CAP, 1.0, 0.0).astype(BF16)
        return dot(pick, zrecv[:, 2048:2176])

    packed_sc = jnp.where(
        lane8 < 2, scalars(row8), jnp.where(lane8 < 4, scalars(row8 + 8), scalars(16 + row8 % 4))
    )
    set_rows(sc, 0, 0, packed_sc)

    got = {}

    def spread(from_q, from_p, to_q, to_p, device):
        got[to_q, to_p] = [
            started(cell(ref, from_q, from_p), cell(ref, to_q, to_p), device) for ref in (sc, xs)
        ]

    def arrived(rq, rp):
        for copy in got[rq, rp]:
            copy.wait_recv()

    def send_q(rp):
        spread(0, rp, 1, rp, along_q(1))
        spread(0, rp, 3, rp, along_q(-1))

    def pass_on(rp):
        by = PASS[rp]
        arrived(2 - by, rp)
        spread(2 - by, rp, 2, rp, along_q(by))

    spread(0, 0, 0, 1, along_p(1))
    spread(0, 0, 0, 3, along_p(-1))
    spread(0, 0, 0, 2, along_p(2))
    send_q(0)
    arrived(0, 1)
    send_q(1)
    ring[2].wait_recv()
    forward(2, 3)
    ring[6].wait_recv()
    forward(6, 5)
    across(2)
    across(6)
    arrived(0, 3)
    send_q(3)
    pass_on(0)
    arrived(0, 2)
    send_q(2)
    spread(0, 2, 2, 2, along_q(2))
    pass_on(1)
    pass_on(3)
    for n in (3, 5):
        ring[n].wait_recv()
        across(n)
    for rp in range(4):
        for rq in (1, 3):
            if rp == 2 or PASS[rp] != 2 - rq:
                arrived(rq, rp)

    for n in (14, 15, 16):
        loads[n].wait()
    for copy in swap:
        copy.wait_recv()

    def operands(start, count):
        rest = xs[start : start + count, 32:40, :].reshape(8 * count, 1024)
        main = [xs[start : start + count, 16 * h : 16 * h + 16, :].reshape(16 * count, 1024) for h in range(2)]
        return [jnp.concatenate([part, rest], axis=0) for part in main]

    def product(pair, w_lo, w_hi):
        lo, hi = dot_nt(pair[0], w_lo), dot_nt(pair[1], w_hi)
        main = lo.shape[0] // 3 * 2
        rest_lo, rest_hi = lo[main:, :], hi[main:, :]
        count = rest_lo.shape[0]
        top = iota((count, 1), 0) % 8 < 4
        rest = jnp.where(top, rest_lo, pltpu.roll(rest_lo, 4, 0)) + jnp.where(
            top, pltpu.roll(rest_hi, count - 4, 0), rest_hi
        )
        return jnp.concatenate([lo[0:main, :] + hi[0:main, :], rest], axis=0)

    def column(start, count, lane):
        tiles = sc[start : start + count].astype(F32)
        main = jnp.concatenate([tiles[:, :, lane : lane + 1], tiles[:, :, lane + 2 : lane + 3]], axis=1)
        rest = tiles[:, :, lane + 4 : lane + 5]
        return jnp.concatenate([main.reshape(16 * count, 1), rest.reshape(8 * count, 1)], axis=0)

    def expert_rows(pair, start, count):
        gate, up = (product(pair, we[t, :, 0:1024], we[t, :, 1024:2048]) for t in range(2))
        return (silu(gate) * up * column(start, count, 0)).astype(BF16)

    def dense_rows(pair, start, count):
        gate, up = (product(pair, wd[t, 0], wd[t, 1]) for t in range(2))
        share = jnp.where(iota(gate.shape, 1) // 24 == column(start, count, 1).astype(jnp.int32), 1.0, 0.5)
        return (silu(gate) * up * (share / (1.0 + jnp.exp(-gate[:, 22:23])))).astype(BF16)

    near = operands(4, 12)
    near_e = expert_rows(near, 4, 12)
    for copy in cross.values():
        copy.wait_recv()
    near_d = dense_rows(near, 4, 12)
    for rp in range(4):
        arrived(2, rp)
    far = operands(0, 4)
    far_e = expert_rows(far, 0, 4)
    far_d = dense_rows(far, 0, 4)

    def down(hidden_e, hidden_d, start, count):
        main = 16 * count
        top = iota((8 * count, 1), 0) % 8 < 4
        for n in range(2):
            cols = slice(512 * n, 512 * n + 512)
            part = [
                dot(hidden_e, we[2, :, 1024 * h + 512 * n : 1024 * h + 512 * n + 512]) + dot(hidden_d, wd[2, h, :, cols])
                for h in range(2)
            ]
            for h in range(2):
                outs[start : start + count, 16 * h : 16 * h + 16, cols] = (
                    part[h][0:main, :].astype(BF16).reshape(count, 16, 512)
                )
            rest = jnp.where(top, part[0][main:, :], part[1][main:, :])
            outs[start : start + count, 32:40, cols] = rest.reshape(count, 8, 512).astype(BF16)

    back = {}

    def at_rp(ref, rp):
        return ref.at[rp]

    def rp_rows(ref, rp):
        return ref[rp].astype(F32)

    down(far_e, far_d, 0, 4)
    direct = started(cell(outs, 2, 2), at_rp(opp_q, 2), along_q(2))
    for rp in (1, 3, 0):
        back[2, rp] = started(cell(outs, 2, rp), at_rp(opp_q, rp), along_q(-PASS[rp]))
    down(near_e, near_d, 4, 12)

    def send_back(rq, rp):
        back[rq, rp] = started(cell(outs, rq, rp), at_rp(fin_q.at[rq // 2], rp), along_q(-1 if rq == 1 else 1))

    for rq, rp in ((1, 2), (3, 2), (1, 1), (3, 1), (1, 3), (3, 3), (1, 0), (3, 0)):
        if rp == 2 or PASS[rp] != 2 - rq:
            send_back(rq, rp)
    for rp in (1, 3, 0):
        rq = 2 - PASS[rp]
        back[2, rp].wait_recv()
        set_rows(outs, rq, rp, cell_rows(outs, rq, rp) + rp_rows(opp_q, rp))
        send_back(rq, rp)

    total = {}

    def sum_q(rp):
        for rq in (1, 3):
            back[rq, rp].wait_recv()
        total[rp] = cell_rows(outs, 0, rp) + rp_rows(fin_q.at[0], rp) + rp_rows(fin_q.at[1], rp)

    def send_p(n, rp, by):
        tsend[n] = total[rp].astype(BF16)
        back["p", n] = started(tsend.at[n], fin_p.at[n], along_p(by))

    sum_q(2)
    direct.wait_recv()
    total[2] = total[2] + rp_rows(opp_q, 2)
    send_p(0, 2, 2)
    sum_q(1)
    send_p(1, 1, -1)
    sum_q(3)
    send_p(2, 3, 1)
    sum_q(0)
    for n in range(3):
        back["p", n].wait_recv()
    summed = (total[0] + rp_rows(fin_p, 0) + rp_rows(fin_p, 1) + rp_rows(fin_p, 2)).astype(BF16)

    for h in range(2):
        rbuf[h] = dot(pack_matrix(iota((32, 40), 1), iota((32, 40), 0), h), summed).astype(BF16)

    def ret_copy(j, h, device):
        d = 4 * c + j
        return pltpu.make_async_remote_copy(
            src_ref=rbuf.at[h, pl.ds(SLOT * j, SLOT)],
            dst_ref=ret.at[pl.ds(pl.multiple_of(SLOT * d, SLOT), SLOT)],
            send_sem=ret_send.at[2 * j + h],
            recv_sem=ret_recv.at[d],
            device_id=device,
            device_id_type=MESH,
        )

    def ret_device(j, h):
        return {**along_z(4 * c + j), "tp": h}

    def ret_each(act):
        @pl.when(first)
        def _():
            for j in (3, 2, 1):
                for h in range(2):
                    act(ret_copy(j, h, ret_device(j, h)))
            act(ret_copy(0, 1, {"tp": 1}))

        @pl.when(jnp.logical_not(first))
        def _():
            for j in range(4):
                for h in range(2):
                    act(ret_copy(j, h, ret_device(j, h)))

    ret_each(lambda copy: copy.start())

    @pl.when(first)
    def _():
        ret[0:SLOT, :] = rbuf[0, 0:SLOT, :]

    def ret_wait(d):
        pltpu.make_async_remote_copy(
            src_ref=rbuf.at[0, pl.ds(0, SLOT)],
            dst_ref=ret.at[pl.ds(SLOT * d, SLOT)],
            send_sem=ret_send.at[0],
            recv_sem=ret_recv.at[d],
            device_id=partner,
            device_id_type=MESH,
        ).wait_recv()

    after_own, _ = halves(after[:, 0:1024], after[:, 1024:2048])
    for d in range(1, 8):
        ret_wait(d)

    @pl.when(jnp.logical_not(first))
    def _():
        ret_wait(0)

    mixed[...] = (after_own + dot_tn(chosen.astype(BF16), ret[...])).astype(BF16)

    for copy in sent:
        copy.wait_send()
    for j in (1, 2, 3):
        moved[j].wait_send()

    @pl.when(jnp.logical_not(first))
    def _():
        moved[0].wait_send()

    ret_each(lambda copy: copy.wait_send())
    assert used[0] <= COPIES


def body(
    tokens,
    state,
    norm_mix,
    w_query,
    w_key,
    w_value,
    w_out,
    norm_ffn,
    gate_vector,
    dense_gate,
    dense_up,
    dense_down,
    exp_gate,
    exp_up,
    exp_down,
    routes,
    route_w,
):
    vmem = pl.BlockSpec(memory_space=pltpu.VMEM)
    hbm = pl.BlockSpec(memory_space=pltpu.HBM)

    def buf(*shape, dtype=BF16):
        return pltpu.VMEM(shape, dtype)

    return pl.pallas_call(
        kernel,
        out_shape=(
            pltpu.VMEM(tokens.shape, tokens.dtype),
            pltpu.VMEM(state.shape, state.dtype),
        ),
        in_specs=[hbm] * 17,
        out_specs=(vmem, vmem),
        scratch_shapes=[
            buf(16, 1024),
            buf(1, 2048, dtype=F32),
            buf(1, 1024, dtype=F32),
            buf(8, 128),
            buf(2, 16, dtype=jnp.int32),
            buf(2, 16),
            buf(22, 1024),
            buf(22, 1024),
            buf(22, 1024),
            buf(2048, 256),
            buf(2048, 256),
            buf(2048, 256),
            buf(256, 2048),
            buf(16, 256, dtype=F32),
            buf(16, 1024),
            buf(1, 1024, dtype=F32),
            buf(16, 2048),
            buf(16, 2048),
            buf(3, 176, 2048),
            buf(3, 2, 168, 1024),
            buf(32, 2176),
            buf(32, 2176),
            buf(16, 40, 1024),
            buf(16, 8, 128),
            buf(16, 40, 1024),
            buf(4, 40, 1024),
            buf(2, 4, 40, 1024),
            buf(3, 40, 1024),
            buf(3, 40, 1024),
            buf(2, 32, 1024),
            buf(64, 1024),
            pltpu.SemaphoreType.DMA((17,)),
            pltpu.SemaphoreType.DMA((COPIES,)),
            pltpu.SemaphoreType.DMA((COPIES,)),
            pltpu.SemaphoreType.DMA((8,)),
            pltpu.SemaphoreType.DMA((8,)),
        ],
        compiler_params=pltpu.CompilerParams(collective_id=0, has_side_effects=True, vmem_limit_bytes=56 * 1024 * 1024),
        name="layer",
    )(
        *(
            pltpu.with_memory_space_constraint(operand, pltpu.HBM)
            for operand in (
                tokens,
                norm_mix.reshape(1, -1),
                norm_ffn.reshape(1, -1),
                gate_vector.reshape(8, 128),
                routes.T,
                route_w.T,
                dense_gate.T,
                dense_up.T,
                dense_down,
                state,
                w_query,
                w_key,
                w_value,
                w_out,
                exp_gate[0].T,
                exp_up[0].T,
                exp_down[0],
            )
        )
    )


def solution(mesh):
    finer = Mesh(mesh.devices.reshape(8, 4, 4, mesh.shape["tp"]), (*EP, "tp"))
    in_specs = (
        P(EP, "tp"),
        P(EP, "tp", None, None),
        P(),
        P(None, "tp"),
        P(None, "tp"),
        P(None, "tp"),
        P("tp", None),
        P("tp"),
        P("tp"),
        P("tp", EP),
        P("tp", EP),
        P(EP, "tp"),
        P(EP, None, "tp"),
        P(EP, None, "tp"),
        P(EP, "tp", None),
        P(EP, None),
        P(EP, None),
    )
    out_specs = (P(EP, "tp"), P(EP, "tp", None, None))
    return jax.shard_map(body, mesh=finer, in_specs=in_specs, out_specs=out_specs, check_vma=False)
```

```python
import jax
import jax.numpy as jnp
from jax import lax
from jax.experimental import pallas as pl
from jax.experimental.pallas import tpu as pltpu
from jax.sharding import Mesh
from jax.sharding import PartitionSpec as P

EP = ("ep_0", "ep_1", "ep_2")
Z, Y, X = EP
MESH = pl.DeviceIdType.MESH
SLOT = 8
CAP = 5
F32 = jnp.float32
BF16 = jnp.bfloat16
epsilon = 1e-06
COPIES = 112
AT = {2: 0, 1: 1, 3: 2, 0: 3}
PASS = {0: -1, 1: 1, 3: -1}


def iota(shape, dim):
    return lax.broadcasted_iota(jnp.int32, shape, dim)


def dot(a, b):
    return jnp.dot(a, b, preferred_element_type=F32)


def dot_nt(a, b):
    return lax.dot_general(a, b, (((1,), (1,)), ((), ())), preferred_element_type=F32)


def dot_tn(a, b):
    return lax.dot_general(a, b, (((0,), (0,)), ((), ())), preferred_element_type=F32)


def silu(v):
    return v / (1.0 + jnp.exp(-v))


def pack_matrix(row, col, half):
    main = row < 32
    slot = jnp.where(main, row % 16, 16 + row % 4)
    part = jnp.where(main, row // 16, (row - 32) // 4)
    return jnp.where((part == half) & (col == slot // CAP * SLOT + slot % CAP), 1.0, 0.0).astype(BF16)


def kernel(
    tokens_h,
    norm_mix_h,
    norm_ffn_h,
    gate_vec_h,
    routes_h,
    route_w_h,
    dgate_h,
    dup_h,
    ddown_h,
    state,
    w_query,
    w_key,
    w_value,
    w_out,
    egate,
    eup,
    edown,
    mixed,
    st,
    tokens,
    norm_mix,
    norm_ffn,
    gate_vec,
    routes,
    route_w,
    dgate,
    dup,
    ddown,
    wq,
    wk,
    wv,
    wo,
    read,
    tok_p,
    nf_p,
    mix_o,
    mix_p,
    we,
    wd,
    disp,
    zrecv,
    xs,
    sc,
    outs,
    opp_q,
    fin_q,
    tsend,
    fin_p,
    rbuf,
    ret,
    local_sem,
    send_sem,
    recv_sem,
    ret_send,
    ret_recv,
    known,
):
    z, y, x, c = (lax.axis_index(a) for a in (Z, Y, X, "tp"))
    first = c == 0
    used = [0]

    def wrap(value, size):
        return lax.rem(value + size, size)

    def along_z(by):
        return {Z: wrap(z + by, 8)}

    def along_p(by):
        return {X: wrap(x + by * (1 - c), 4), Y: wrap(y + by * c, 4)}

    def along_q(by):
        return {X: wrap(x + by * c, 4), Y: wrap(y + by * (1 - c), 4)}

    partner = {"tp": 1 - c}

    def remote(src, dst, device):
        n = used[0]
        used[0] += 1
        return pltpu.make_async_remote_copy(
            src_ref=src,
            dst_ref=dst,
            send_sem=send_sem.at[n],
            recv_sem=recv_sem.at[n],
            device_id=device,
            device_id_type=MESH,
        )

    sent = []

    def started(src, dst, device):
        copy = remote(src, dst, device)
        copy.start()
        sent.append(copy)
        return copy

    def halves(own, other):
        return jnp.where(first, own, other), jnp.where(first, other, own)

    def as_row(ref):
        rows = ref[...].astype(F32)
        return jnp.concatenate([rows[i : i + 1, :] for i in range(8)], axis=1)

    loads = {}
    for n, (src, dst) in enumerate(
        [
            (tokens_h, tokens),
            (norm_ffn_h, norm_ffn),
            (dgate_h, dgate),
            (dup_h, dup),
            (ddown_h, ddown),
            (gate_vec_h, gate_vec),
            (norm_mix_h, norm_mix),
            (routes_h, routes),
            (route_w_h, route_w),
            (w_query, wq),
            (w_key, wk),
            (w_value, wv),
            (state, st),
            (w_out, wo),
            (egate, we.at[0, pl.ds(0, 88)]),
            (eup, we.at[1, pl.ds(0, 88)]),
            (edown, we.at[2, pl.ds(0, 88)]),
        ]
    ):
        loads[n] = pltpu.make_async_copy(src, dst, local_sem.at[n])
        loads[n].start()

    barrier = pltpu.get_barrier_semaphore()
    peers = [partner]
    for by in (1, -1):
        peers += [along_z(by), along_p(by), along_q(by)]
    for peer in peers:
        pl.semaphore_signal(barrier, inc=1, device_id=peer, device_id_type=MESH)

    for n in range(9):
        loads[n].wait()
    tail = jnp.zeros((2, 1024), F32)
    gate_tail = jnp.concatenate([as_row(gate_vec), tail[0:1, :]], axis=0)
    for t, (ref, end) in enumerate(((dgate, gate_tail), (dup, tail), (ddown, tail))):
        block = jnp.concatenate([ref[...].astype(F32), end], axis=0)
        wd[t, pl.ds(c, 1), pl.ds(0, 24), :] = block.astype(BF16)[None]

    pl.semaphore_wait(barrier, len(peers))

    def tell(n, device):
        pl.semaphore_signal(known.at[n], inc=1, device_id=device, device_id_type=MESH)

    def hear(n):
        pl.semaphore_wait(known.at[n], 1)

    tell(0, along_z(1))
    tell(3, along_z(-1))
    tell(6, along_p(1))
    tell(7, along_q(1))

    def relay(n):
        for start, by in ((0, 1), (3, -1)):
            hear(start + n)
            tell(start + n + 1, along_z(by))


    pair = [started(tokens, tok_p, partner), started(norm_ffn, nf_p, partner)]

    def wd_slot(n):
        return wd.at[:, pl.ds(c, 1), pl.ds(24 * (n - (n > 4)), 24), :]

    ring, cross = {}, {}

    def forward(source, target):
        ring[target] = started(wd_slot(source), wd_slot(target), along_z(1 if target < 4 else -1))

    def across(n):
        cross[n] = started(wd_slot(n), wd_slot(n), partner)

    forward(0, 1)
    forward(0, 7)
    swap = [started(src, we.at[t, pl.ds(88, 88)], partner) for t, src in enumerate((egate, eup, edown))]
    across(0)

    for copy in pair:
        copy.wait_recv()
    lo, hi = halves(tokens[...].astype(F32), tok_p[...].astype(F32))
    full = jnp.concatenate([lo, hi], axis=1)
    mean = jnp.sum(full * full, axis=1, keepdims=True) / 2048.0
    normed = (full * lax.rsqrt(mean + epsilon) * norm_mix[...]).astype(BF16)
    for n in (9, 10, 11):
        loads[n].wait()
    query = dot(normed, wq[...]).astype(BF16).astype(F32)
    key = dot(normed, wk[...]).astype(BF16).astype(F32) * 128 ** (-0.5)
    value = dot(normed, wv[...]).astype(BF16).astype(F32)
    blank = jnp.zeros((112, 256), F32)
    query_t = jnp.concatenate([query, blank], axis=0).T
    key_t = jnp.concatenate([key, blank], axis=0).T
    relay(0)
    loads[12].wait()
    decay = [jnp.where(first, 1.0 - 2.0 ** (-3.0 - 2.0 * h), 1.0 - 2.0 ** (-7.0 - 2.0 * h)) for h in range(2)]
    for h in range(2):
        span = slice(128 * h, 128 * h + 128)
        for s in range(16):
            read[s : s + 1, span] = jnp.sum(query_t[span, s : s + 1] * st[s, h], axis=0, keepdims=True)
    heads = []
    for h in range(2):
        span = slice(128 * h, 128 * h + 128)
        met = jnp.sum(query[:, span] * key[:, span], axis=1, keepdims=True)
        part = decay[h] * read[:, span] + met * value[:, span]
        centre = jnp.mean(part, axis=1, keepdims=True)
        spread = jnp.mean(jnp.square(part - centre), axis=1, keepdims=True)
        heads.append(((part - centre) * lax.rsqrt(spread + epsilon)).astype(BF16))
    loads[13].wait()
    mix = dot(heads[0], wo[0:128, :]) + dot(heads[1], wo[128:256, :])
    mix_o[...] = mix.astype(BF16)
    mix_copy = started(mix_o, mix_p, partner)

    block = iota((64, 16), 0)
    expert = lax.rem(z - block // SLOT + 8, 8)
    hit0 = jnp.where(routes[0:1, :] == expert, 1.0, 0.0)
    hit1 = jnp.where(routes[1:2, :] == expert, 1.0, 0.0)
    member = hit0 + hit1
    before = jnp.where(iota((16, 16), 0) < iota((16, 16), 1), 1.0, 0.0).astype(BF16)
    place = dot(member.astype(BF16), before)
    chosen = jnp.where(place == (block % SLOT).astype(F32), member, 0.0)
    weights = route_w[...].astype(F32)
    slot_w = jnp.sum(chosen * (hit0 * weights[0:1, :] + hit1 * weights[1:2, :]), axis=1, keepdims=True)
    other = jnp.where(hit0 > 0.0, routes[1:2, :], routes[0:1, :])
    absent = lax.rem(expert - other + 12, 8)
    absent = jnp.where(absent > 4, absent - 1, absent).astype(F32)
    slot_absent = jnp.sum(chosen * absent, axis=1, keepdims=True)
    extra = jnp.where(iota((64, 128), 1) % 2 == 0, slot_w, slot_absent)
    extra = jnp.where(first, extra[0:32, :], extra[32:64, :]).astype(BF16)
    mine = jnp.where(first, chosen[0:32, :], chosen[32:64, :]).astype(BF16)

    relay(1)
    mix_copy.wait_recv()
    after = (full + (mix_o[...].astype(F32) + mix_p[...].astype(F32))).astype(BF16).astype(F32)
    mean2 = jnp.sum(after * after, axis=1, keepdims=True) / 2048.0
    nf_lo, nf_hi = halves(norm_ffn[...], nf_p[...])
    normed2 = (after * lax.rsqrt(mean2 + epsilon) * jnp.concatenate([nf_lo, nf_hi], axis=1)).astype(BF16)

    hear(2)
    hear(5)
    rows = dot(mine, normed2)
    disp[:, 2048:2176] = extra
    disp[:, 0:2048] = rows.astype(BF16)
    moved = []
    for j in range(4):
        part = pl.ds(SLOT * j, SLOT)
        moved.append(remote(disp.at[part], zrecv.at[part], along_z(-(4 * c + j))))

    @pl.when(first)
    def _():
        for j in (3, 2, 1):
            moved[j].start()
        zrecv[0:SLOT, :] = disp[0:SLOT, :]

    @pl.when(jnp.logical_not(first))
    def _():
        for j in range(4):
            moved[j].start()

    for h in range(2):
        span = slice(128 * h, 128 * h + 128)
        for s in range(16):
            st[s, h] = decay[h] * st[s, h] + key_t[span, s : s + 1] * value[s : s + 1, span]

    ring[1].wait_recv()
    forward(1, 2)
    ring[7].wait_recv()
    forward(7, 6)
    across(1)
    across(7)
    for j in (1, 2, 3):
        moved[j].wait_recv()

    @pl.when(jnp.logical_not(first))
    def _():
        moved[0].wait_recv()

    def cell(ref, rq, rp):
        return ref.at[4 * AT[rq] + rp]

    def cell_rows(ref, rq, rp):
        return ref[4 * AT[rq] + rp].astype(F32)

    def set_rows(ref, rq, rp, rows):
        ref[4 * AT[rq] + rp] = rows.astype(BF16)

    row, col = iota((40, 32), 0), iota((40, 32), 1)
    packed = dot(pack_matrix(row, col, 0), zrecv[:, 0:1024]) + dot(pack_matrix(row, col, 1), zrecv[:, 1024:2048])
    set_rows(xs, 0, 0, packed)
    lane8, row8, col8 = iota((8, 128), 1), iota((8, 32), 0), iota((8, 32), 1)

    def scalars(slot):
        pick = jnp.where(col8 == slot // CAP * SLOT + slot % CAP, 1.0, 0.0).astype(BF16)
        return dot(pick, zrecv[:, 2048:2176])

    packed_sc = jnp.where(
        lane8 < 2, scalars(row8), jnp.where(lane8 < 4, scalars(row8 + 8), scalars(16 + row8 % 4))
    )
    set_rows(sc, 0, 0, packed_sc)

    got = {}

    def chunk(ref, rq, rp, n):
        return ref.at[4 * AT[rq] + rp, :, pl.ds(512 * n, 512)]

    def spread(from_q, from_p, to_q, to_p, n, device):
        got[to_q, to_p, n] = started(chunk(xs, from_q, from_p, n), chunk(xs, to_q, to_p, n), device)
        if n == 0:
            got[to_q, to_p, 2] = started(cell(sc, from_q, from_p), cell(sc, to_q, to_p), device)

    def arrived(rq, rp, n):
        got[rq, rp, n].wait_recv()
        if n == 0:
            got[rq, rp, 2].wait_recv()

    def send_q(rp, n):
        spread(0, rp, 1, rp, n, along_q(1))
        spread(0, rp, 3, rp, n, along_q(-1))

    def pass_on(rp, n):
        by = PASS[rp]
        arrived(2 - by, rp, n)
        spread(2 - by, rp, 2, rp, n, along_q(by))

    hear(6)
    hear(7)
    for n in range(2):
        spread(0, 0, 0, 1, n, along_p(1))
        spread(0, 0, 0, 3, n, along_p(-1))
        send_q(0, n)
        spread(0, 0, 0, 2, n, along_p(2))
    for n in range(2):
        arrived(0, 1, n)
        send_q(1, n)
        arrived(0, 3, n)
        send_q(3, n)
        pass_on(0, n)
    for n in range(2):
        arrived(0, 2, n)
        send_q(2, n)
        spread(0, 2, 2, 2, n, along_q(2))
    ring[2].wait_recv()
    forward(2, 3)
    ring[6].wait_recv()
    forward(6, 5)
    across(2)
    across(6)
    for n in (14, 15, 16):
        loads[n].wait()
    for copy in swap:
        copy.wait_recv()

    def operands(start, count):
        rest = xs[start : start + count, 32:40, :].reshape(8 * count, 1024)
        main = [xs[start : start + count, 16 * h : 16 * h + 16, :].reshape(16 * count, 1024) for h in range(2)]
        return [jnp.concatenate([part, rest], axis=0) for part in main]

    def product(pair, w_lo, w_hi):
        lo, hi = dot_nt(pair[0], w_lo), dot_nt(pair[1], w_hi)
        main = lo.shape[0] // 3 * 2
        rest_lo, rest_hi = lo[main:, :], hi[main:, :]
        count = rest_lo.shape[0]
        top = iota((count, 1), 0) % 8 < 4
        rest = jnp.where(top, rest_lo, pltpu.roll(rest_lo, 4, 0)) + jnp.where(
            top, pltpu.roll(rest_hi, count - 4, 0), rest_hi
        )
        return jnp.concatenate([lo[0:main, :] + hi[0:main, :], rest], axis=0)

    def column(start, count, lane):
        tiles = sc[start : start + count].astype(F32)
        main = jnp.concatenate([tiles[:, :, lane : lane + 1], tiles[:, :, lane + 2 : lane + 3]], axis=1)
        rest = tiles[:, :, lane + 4 : lane + 5]
        return jnp.concatenate([main.reshape(16 * count, 1), rest.reshape(8 * count, 1)], axis=0)

    def expert_rows(pair, start, count):
        gate, up = (product(pair, we[t, :, 0:1024], we[t, :, 1024:2048]) for t in range(2))
        return (silu(gate) * up * column(start, count, 0)).astype(BF16)

    def dense_rows(pair, start, count):
        gate, up = (product(pair, wd[t, 0], wd[t, 1]) for t in range(2))
        share = jnp.where(iota(gate.shape, 1) // 24 == column(start, count, 1).astype(jnp.int32), 1.0, 0.5)
        return (silu(gate) * up * (share / (1.0 + jnp.exp(-gate[:, 22:23])))).astype(BF16)

    own = operands(12, 4)
    own_e = expert_rows(own, 12, 4)
    for n in range(2):
        pass_on(1, n)
        pass_on(3, n)
    for n in (3, 5):
        ring[n].wait_recv()
        across(n)
    for copy in cross.values():
        copy.wait_recv()
    own_d = dense_rows(own, 12, 4)
    for n in range(2):
        for rp in range(4):
            for rq in (1, 3):
                if rp == 2 or PASS[rp] != 2 - rq:
                    arrived(rq, rp, n)
    for n in range(2):
        for rp in range(4):
            arrived(2, rp, n)
    rest = operands(0, 12)
    rest_e = expert_rows(rest, 0, 12)
    rest_d = dense_rows(rest, 0, 12)

    def blocks(rows, start, count):
        return jnp.concatenate(
            [rows[16 * start : 16 * (start + count), :], rows[192 + 8 * start : 192 + 8 * (start + count), :]], axis=0
        )

    def down(hidden_e, hidden_d, start, count, then):
        main = 16 * count
        top = iota((8 * count, 1), 0) % 8 < 4
        for n in range(2):
            cols = slice(512 * n, 512 * n + 512)
            part = [
                dot(hidden_e, we[2, :, 1024 * h + 512 * n : 1024 * h + 512 * n + 512]) + dot(hidden_d, wd[2, h, :, cols])
                for h in range(2)
            ]
            for h in range(2):
                outs[start : start + count, 16 * h : 16 * h + 16, cols] = (
                    part[h][0:main, :].astype(BF16).reshape(count, 16, 512)
                )
            rest = jnp.where(top, part[0][main:, :], part[1][main:, :])
            outs[start : start + count, 32:40, cols] = rest.reshape(count, 8, 512).astype(BF16)
            then(n)

    back = {}

    def part(ref, rp, n):
        return ref.at[rp, :, pl.ds(512 * n, 512)]

    def part_rows(ref, rp, n):
        return ref[rp, :, 512 * n : 512 * n + 512].astype(F32)

    def send_far(n):
        back["far", n] = started(chunk(outs, 2, 2, n), part(opp_q, 2, n), along_q(2))
        for rp in (1, 3, 0):
            back[2, rp, n] = started(chunk(outs, 2, rp, n), part(opp_q, rp, n), along_q(-PASS[rp]))

    def send_back(rq, rp, n):
        device = along_q(-1 if rq == 1 else 1)
        back[rq, rp, n] = started(chunk(outs, rq, rp, n), part(fin_q.at[rq // 2], rp, n), device)

    def send_near(n):
        for rq, rp in ((1, 2), (3, 2), (1, 1), (3, 1), (1, 3), (3, 3), (1, 0), (3, 0)):
            if rp == 2 or PASS[rp] != 2 - rq:
                send_back(rq, rp, n)

    down(blocks(rest_e, 0, 4), blocks(rest_d, 0, 4), 0, 4, send_far)
    down(blocks(rest_e, 4, 8), blocks(rest_d, 4, 8), 4, 8, send_near)
    down(own_e, own_d, 12, 4, lambda n: None)
    for n in range(2):
        for rp in (1, 3, 0):
            rq = 2 - PASS[rp]
            at = 4 * AT[rq] + rp
            back[2, rp, n].wait_recv()
            both = part_rows(outs, at, n) + part_rows(opp_q, rp, n)
            outs[at, :, 512 * n : 512 * n + 512] = both.astype(BF16)
            send_back(rq, rp, n)

    total = {}

    def sum_q(rp, n):
        for rq in (1, 3):
            back[rq, rp, n].wait_recv()
        own_part = part_rows(outs, 4 * AT[0] + rp, n)
        total[rp, n] = own_part + part_rows(fin_q.at[0], rp, n) + part_rows(fin_q.at[1], rp, n)

    def send_p(slot, rp, n, by):
        tsend[slot, :, 512 * n : 512 * n + 512] = total[rp, n].astype(BF16)
        back["p", slot, n] = started(part(tsend, slot, n), part(fin_p, slot, n), along_p(by))

    for n in range(2):
        sum_q(2, n)
        back["far", n].wait_recv()
        total[2, n] = total[2, n] + part_rows(opp_q, 2, n)
        send_p(0, 2, n, 2)
    for n in range(2):
        sum_q(1, n)
        send_p(1, 1, n, -1)
        sum_q(3, n)
        send_p(2, 3, n, 1)
    for n in range(2):
        sum_q(0, n)
    ends = []
    for n in range(2):
        for slot in range(3):
            back["p", slot, n].wait_recv()
        ends.append(total[0, n] + part_rows(fin_p, 0, n) + part_rows(fin_p, 1, n) + part_rows(fin_p, 2, n))
    summed = jnp.concatenate(ends, axis=1).astype(BF16)

    for h in range(2):
        rbuf[h] = dot(pack_matrix(iota((32, 40), 1), iota((32, 40), 0), h), summed).astype(BF16)

    def ret_copy(j, h, device):
        d = 4 * c + j
        return pltpu.make_async_remote_copy(
            src_ref=rbuf.at[h, pl.ds(SLOT * j, SLOT)],
            dst_ref=ret.at[pl.ds(pl.multiple_of(SLOT * d, SLOT), SLOT)],
            send_sem=ret_send.at[2 * j + h],
            recv_sem=ret_recv.at[d],
            device_id=device,
            device_id_type=MESH,
        )

    def ret_device(j, h):
        return {**along_z(4 * c + j), "tp": h}

    def ret_each(act):
        @pl.when(first)
        def _():
            for j in (3, 2, 1):
                for h in range(2):
                    act(ret_copy(j, h, ret_device(j, h)))
            act(ret_copy(0, 1, {"tp": 1}))

        @pl.when(jnp.logical_not(first))
        def _():
            for j in range(4):
                for h in range(2):
                    act(ret_copy(j, h, ret_device(j, h)))

    ret_each(lambda copy: copy.start())

    @pl.when(first)
    def _():
        ret[0:SLOT, :] = rbuf[0, 0:SLOT, :]

    def ret_wait(d):
        pltpu.make_async_remote_copy(
            src_ref=rbuf.at[0, pl.ds(0, SLOT)],
            dst_ref=ret.at[pl.ds(SLOT * d, SLOT)],
            send_sem=ret_send.at[0],
            recv_sem=ret_recv.at[d],
            device_id=partner,
            device_id_type=MESH,
        ).wait_recv()

    after_own, _ = halves(after[:, 0:1024], after[:, 1024:2048])
    for d in range(1, 8):
        ret_wait(d)

    @pl.when(jnp.logical_not(first))
    def _():
        ret_wait(0)

    mixed[...] = (after_own + dot_tn(chosen.astype(BF16), ret[...])).astype(BF16)

    for copy in sent:
        copy.wait_send()
    for j in (1, 2, 3):
        moved[j].wait_send()

    @pl.when(jnp.logical_not(first))
    def _():
        moved[0].wait_send()

    ret_each(lambda copy: copy.wait_send())
    assert used[0] <= COPIES


def body(
    tokens,
    state,
    norm_mix,
    w_query,
    w_key,
    w_value,
    w_out,
    norm_ffn,
    gate_vector,
    dense_gate,
    dense_up,
    dense_down,
    exp_gate,
    exp_up,
    exp_down,
    routes,
    route_w,
):
    vmem = pl.BlockSpec(memory_space=pltpu.VMEM)
    hbm = pl.BlockSpec(memory_space=pltpu.HBM)

    def buf(*shape, dtype=BF16):
        return pltpu.VMEM(shape, dtype)

    return pl.pallas_call(
        kernel,
        out_shape=(
            pltpu.VMEM(tokens.shape, tokens.dtype),
            pltpu.VMEM(state.shape, state.dtype),
        ),
        in_specs=[hbm] * 17,
        out_specs=(vmem, vmem),
        scratch_shapes=[
            buf(16, 1024),
            buf(1, 2048, dtype=F32),
            buf(1, 1024, dtype=F32),
            buf(8, 128),
            buf(2, 16, dtype=jnp.int32),
            buf(2, 16),
            buf(22, 1024),
            buf(22, 1024),
            buf(22, 1024),
            buf(2048, 256),
            buf(2048, 256),
            buf(2048, 256),
            buf(256, 2048),
            buf(16, 256, dtype=F32),
            buf(16, 1024),
            buf(1, 1024, dtype=F32),
            buf(16, 2048),
            buf(16, 2048),
            buf(3, 176, 2048),
            buf(3, 2, 168, 1024),
            buf(32, 2176),
            buf(32, 2176),
            buf(16, 40, 1024),
            buf(16, 8, 128),
            buf(16, 40, 1024),
            buf(4, 40, 1024),
            buf(2, 4, 40, 1024),
            buf(3, 40, 1024),
            buf(3, 40, 1024),
            buf(2, 32, 1024),
            buf(64, 1024),
            pltpu.SemaphoreType.DMA((17,)),
            pltpu.SemaphoreType.DMA((COPIES,)),
            pltpu.SemaphoreType.DMA((COPIES,)),
            pltpu.SemaphoreType.DMA((8,)),
            pltpu.SemaphoreType.DMA((8,)),
            pltpu.SemaphoreType.REGULAR((8,)),
        ],
        compiler_params=pltpu.CompilerParams(collective_id=0, has_side_effects=True, vmem_limit_bytes=56 * 1024 * 1024),
        name="layer",
    )(
        *(
            pltpu.with_memory_space_constraint(operand, pltpu.HBM)
            for operand in (
                tokens,
                norm_mix.reshape(1, -1),
                norm_ffn.reshape(1, -1),
                gate_vector.reshape(8, 128),
                routes.T,
                route_w.T,
                dense_gate.T,
                dense_up.T,
                dense_down,
                state,
                w_query,
                w_key,
                w_value,
                w_out,
                exp_gate[0].T,
                exp_up[0].T,
                exp_down[0],
            )
        )
    )


def solution(mesh):
    finer = Mesh(mesh.devices.reshape(8, 4, 4, mesh.shape["tp"]), (*EP, "tp"))
    in_specs = (
        P(EP, "tp"),
        P(EP, "tp", None, None),
        P(),
        P(None, "tp"),
        P(None, "tp"),
        P(None, "tp"),
        P("tp", None),
        P("tp"),
        P("tp"),
        P("tp", EP),
        P("tp", EP),
        P(EP, "tp"),
        P(EP, None, "tp"),
        P(EP, None, "tp"),
        P(EP, "tp", None),
        P(EP, None),
        P(EP, None),
    )
    out_specs = (P(EP, "tp"), P(EP, "tp", None, None))
    return jax.shard_map(body, mesh=finer, in_specs=in_specs, out_specs=out_specs, check_vma=False)
```

```python
import jax
import jax.numpy as jnp
from jax import lax
from jax.experimental import pallas as pl
from jax.experimental.pallas import tpu as pltpu
from jax.sharding import Mesh
from jax.sharding import PartitionSpec as P

EP = ("ep_0", "ep_1", "ep_2")
Z, Y, X = EP
MESH = pl.DeviceIdType.MESH
SLOT = 8
CAP = 5
F32 = jnp.float32
BF16 = jnp.bfloat16
epsilon = 1e-06
COPIES = 112
AT = {2: 0, 1: 1, 3: 2, 0: 3}
PASS = {0: -1, 1: 1, 3: -1}


def iota(shape, dim):
    return lax.broadcasted_iota(jnp.int32, shape, dim)


def dot(a, b):
    return jnp.dot(a, b, preferred_element_type=F32)


def dot_nt(a, b):
    return lax.dot_general(a, b, (((1,), (1,)), ((), ())), preferred_element_type=F32)


def dot_tn(a, b):
    return lax.dot_general(a, b, (((0,), (0,)), ((), ())), preferred_element_type=F32)


def silu(v):
    return v / (1.0 + jnp.exp(-v))


def pack_matrix(row, col, half):
    main = row < 32
    slot = jnp.where(main, row % 16, 16 + row % 4)
    part = jnp.where(main, row // 16, (row - 32) // 4)
    return jnp.where((part == half) & (col == slot // CAP * SLOT + slot % CAP), 1.0, 0.0).astype(BF16)


def kernel(
    tokens_h,
    norm_mix_h,
    norm_ffn_h,
    gate_vec_h,
    routes_h,
    route_w_h,
    dgate_h,
    dup_h,
    ddown_h,
    state,
    w_query,
    w_key,
    w_value,
    w_out,
    egate,
    eup,
    edown,
    mixed,
    st,
    tokens,
    norm_mix,
    norm_ffn,
    gate_vec,
    routes,
    route_w,
    dgate,
    dup,
    ddown,
    wq,
    wk,
    wv,
    wo,
    read,
    tok_p,
    nf_p,
    mix_o,
    mix_p,
    we,
    wd,
    disp,
    zrecv,
    xs,
    sc,
    outs,
    opp_q,
    fin_q,
    tsend,
    fin_p,
    rbuf,
    ret,
    local_sem,
    send_sem,
    recv_sem,
    ret_send,
    ret_recv,
    known,
):
    z, y, x, c = (lax.axis_index(a) for a in (Z, Y, X, "tp"))
    first = c == 0
    used = [0]

    def wrap(value, size):
        return lax.rem(value + size, size)

    def along_z(by):
        return {Z: wrap(z + by, 8)}

    def along_p(by):
        return {X: wrap(x + by * (1 - c), 4), Y: wrap(y + by * c, 4)}

    def along_q(by):
        return {X: wrap(x + by * c, 4), Y: wrap(y + by * (1 - c), 4)}

    partner = {"tp": 1 - c}

    def remote(src, dst, device):
        n = used[0]
        used[0] += 1
        return pltpu.make_async_remote_copy(
            src_ref=src,
            dst_ref=dst,
            send_sem=send_sem.at[n],
            recv_sem=recv_sem.at[n],
            device_id=device,
            device_id_type=MESH,
        )

    sent = []

    def started(src, dst, device):
        copy = remote(src, dst, device)
        copy.start()
        sent.append(copy)
        return copy

    def halves(own, other):
        return jnp.where(first, own, other), jnp.where(first, other, own)

    def as_row(ref):
        rows = ref[...].astype(F32)
        return jnp.concatenate([rows[i : i + 1, :] for i in range(8)], axis=1)

    loads = {}
    for n, (src, dst) in enumerate(
        [
            (tokens_h, tokens),
            (norm_ffn_h, norm_ffn),
            (dgate_h, dgate),
            (dup_h, dup),
            (ddown_h, ddown),
            (gate_vec_h, gate_vec),
            (norm_mix_h, norm_mix),
            (routes_h, routes),
            (route_w_h, route_w),
            (w_query, wq),
            (w_key, wk),
            (w_value, wv),
            (state, st),
            (w_out, wo),
            (egate, we.at[0, pl.ds(0, 88)]),
            (eup, we.at[1, pl.ds(0, 88)]),
            (edown, we.at[2, pl.ds(0, 88)]),
        ]
    ):
        loads[n] = pltpu.make_async_copy(src, dst, local_sem.at[n])
        loads[n].start()

    barrier = pltpu.get_barrier_semaphore()
    peers = [partner]
    for by in (1, -1):
        peers += [along_z(by), along_z(2 * by), along_p(by), along_q(by)]
    for peer in peers:
        pl.semaphore_signal(barrier, inc=1, device_id=peer, device_id_type=MESH)

    for n in range(9):
        loads[n].wait()
    tail = jnp.zeros((2, 1024), F32)
    gate_tail = jnp.concatenate([as_row(gate_vec), tail[0:1, :]], axis=0)
    for t, (ref, end) in enumerate(((dgate, gate_tail), (dup, tail), (ddown, tail))):
        block = jnp.concatenate([ref[...].astype(F32), end], axis=0)
        wd[t, pl.ds(c, 1), pl.ds(0, 24), :] = block.astype(BF16)[None]

    pl.semaphore_wait(barrier, len(peers))

    def tell(n, device):
        pl.semaphore_signal(known.at[n], inc=1, device_id=device, device_id_type=MESH)

    def hear(n):
        pl.semaphore_wait(known.at[n], 1)

    tell(0, along_z(2))
    tell(1, along_z(-2))
    tell(2, along_p(1))
    tell(3, along_q(1))

    pair = [started(tokens, tok_p, partner), started(norm_ffn, nf_p, partner)]

    def wd_slot(n):
        return wd.at[:, pl.ds(c, 1), pl.ds(24 * (n - (n > 4)), 24), :]

    ring, cross = {}, {}

    def forward(source, target):
        ring[target] = started(wd_slot(source), wd_slot(target), along_z(1 if target < 4 else -1))

    def across(n):
        cross[n] = started(wd_slot(n), wd_slot(n), partner)

    forward(0, 1)
    forward(0, 7)
    swap = [started(src, we.at[t, pl.ds(88, 88)], partner) for t, src in enumerate((egate, eup, edown))]
    across(0)

    for copy in pair:
        copy.wait_recv()
    lo, hi = halves(tokens[...].astype(F32), tok_p[...].astype(F32))
    full = jnp.concatenate([lo, hi], axis=1)
    mean = jnp.sum(full * full, axis=1, keepdims=True) / 2048.0
    normed = (full * lax.rsqrt(mean + epsilon) * norm_mix[...]).astype(BF16)
    for n in (9, 10, 11):
        loads[n].wait()
    query = dot(normed, wq[...]).astype(BF16).astype(F32)
    key = dot(normed, wk[...]).astype(BF16).astype(F32) * 128 ** (-0.5)
    value = dot(normed, wv[...]).astype(BF16).astype(F32)
    blank = jnp.zeros((112, 256), F32)
    query_t = jnp.concatenate([query, blank], axis=0).T
    key_t = jnp.concatenate([key, blank], axis=0).T
    loads[12].wait()
    decay = [jnp.where(first, 1.0 - 2.0 ** (-3.0 - 2.0 * h), 1.0 - 2.0 ** (-7.0 - 2.0 * h)) for h in range(2)]
    for h in range(2):
        span = slice(128 * h, 128 * h + 128)
        for s in range(16):
            read[s : s + 1, span] = jnp.sum(query_t[span, s : s + 1] * st[s, h], axis=0, keepdims=True)
    heads = []
    for h in range(2):
        span = slice(128 * h, 128 * h + 128)
        met = jnp.sum(query[:, span] * key[:, span], axis=1, keepdims=True)
        part = decay[h] * read[:, span] + met * value[:, span]
        centre = jnp.mean(part, axis=1, keepdims=True)
        spread = jnp.mean(jnp.square(part - centre), axis=1, keepdims=True)
        heads.append(((part - centre) * lax.rsqrt(spread + epsilon)).astype(BF16))
    loads[13].wait()
    mix = dot(heads[0], wo[0:128, :]) + dot(heads[1], wo[128:256, :])
    mix_o[...] = mix.astype(BF16)
    mix_copy = started(mix_o, mix_p, partner)

    block = iota((64, 16), 0)
    expert = lax.rem(z - block // SLOT + 8, 8)
    hit0 = jnp.where(routes[0:1, :] == expert, 1.0, 0.0)
    hit1 = jnp.where(routes[1:2, :] == expert, 1.0, 0.0)
    member = hit0 + hit1
    before = jnp.where(iota((16, 16), 0) < iota((16, 16), 1), 1.0, 0.0).astype(BF16)
    place = dot(member.astype(BF16), before)
    chosen = jnp.where(place == (block % SLOT).astype(F32), member, 0.0)
    weights = route_w[...].astype(F32)
    slot_w = jnp.sum(chosen * (hit0 * weights[0:1, :] + hit1 * weights[1:2, :]), axis=1, keepdims=True)
    other = jnp.where(hit0 > 0.0, routes[1:2, :], routes[0:1, :])
    absent = lax.rem(expert - other + 12, 8)
    absent = jnp.where(absent > 4, absent - 1, absent).astype(F32)
    slot_absent = jnp.sum(chosen * absent, axis=1, keepdims=True)
    extra = jnp.where(iota((64, 128), 1) % 2 == 0, slot_w, slot_absent)
    extra = jnp.where(first, extra[0:32, :], extra[32:64, :]).astype(BF16)
    mine = jnp.where(first, chosen[0:32, :], chosen[32:64, :]).astype(BF16)

    mix_copy.wait_recv()
    after = (full + (mix_o[...].astype(F32) + mix_p[...].astype(F32))).astype(BF16).astype(F32)
    mean2 = jnp.sum(after * after, axis=1, keepdims=True) / 2048.0
    nf_lo, nf_hi = halves(norm_ffn[...], nf_p[...])
    normed2 = (after * lax.rsqrt(mean2 + epsilon) * jnp.concatenate([nf_lo, nf_hi], axis=1)).astype(BF16)

    hear(0)
    hear(1)
    rows = dot(mine, normed2)
    disp[:, 2048:2176] = extra
    disp[:, 0:2048] = rows.astype(BF16)
    moved = []
    for j in range(4):
        part = pl.ds(SLOT * j, SLOT)
        moved.append(remote(disp.at[part], zrecv.at[part], along_z(-(4 * c + j))))

    @pl.when(first)
    def _():
        for j in (3, 2, 1):
            moved[j].start()
        zrecv[0:SLOT, :] = disp[0:SLOT, :]

    @pl.when(jnp.logical_not(first))
    def _():
        for j in range(4):
            moved[j].start()

    for h in range(2):
        span = slice(128 * h, 128 * h + 128)
        for s in range(16):
            st[s, h] = decay[h] * st[s, h] + key_t[span, s : s + 1] * value[s : s + 1, span]

    for j in (1, 2, 3):
        moved[j].wait_recv()

    @pl.when(jnp.logical_not(first))
    def _():
        moved[0].wait_recv()

    ring[1].wait_recv()
    forward(1, 2)
    ring[7].wait_recv()
    forward(7, 6)
    across(1)
    across(7)
    def cell(ref, rq, rp):
        return ref.at[4 * AT[rq] + rp]

    def cell_rows(ref, rq, rp):
        return ref[4 * AT[rq] + rp].astype(F32)

    def set_rows(ref, rq, rp, rows):
        ref[4 * AT[rq] + rp] = rows.astype(BF16)

    row, col = iota((40, 32), 0), iota((40, 32), 1)
    packed = dot(pack_matrix(row, col, 0), zrecv[:, 0:1024]) + dot(pack_matrix(row, col, 1), zrecv[:, 1024:2048])
    set_rows(xs, 0, 0, packed)
    lane8, row8, col8 = iota((8, 128), 1), iota((8, 32), 0), iota((8, 32), 1)

    def scalars(slot):
        pick = jnp.where(col8 == slot // CAP * SLOT + slot % CAP, 1.0, 0.0).astype(BF16)
        return dot(pick, zrecv[:, 2048:2176])

    packed_sc = jnp.where(
        lane8 < 2, scalars(row8), jnp.where(lane8 < 4, scalars(row8 + 8), scalars(16 + row8 % 4))
    )
    set_rows(sc, 0, 0, packed_sc)

    got = {}

    def chunk(ref, rq, rp, n):
        return ref.at[4 * AT[rq] + rp, :, pl.ds(512 * n, 512)]

    def spread(from_q, from_p, to_q, to_p, n, device):
        got[to_q, to_p, n] = started(chunk(xs, from_q, from_p, n), chunk(xs, to_q, to_p, n), device)
        if n == 0:
            got[to_q, to_p, 2] = started(cell(sc, from_q, from_p), cell(sc, to_q, to_p), device)

    def arrived(rq, rp, n):
        got[rq, rp, n].wait_recv()
        if n == 0:
            got[rq, rp, 2].wait_recv()

    def send_q(rp, n):
        spread(0, rp, 1, rp, n, along_q(1))
        spread(0, rp, 3, rp, n, along_q(-1))

    def pass_on(rp, n):
        by = PASS[rp]
        arrived(2 - by, rp, n)
        spread(2 - by, rp, 2, rp, n, along_q(by))

    hear(2)
    hear(3)
    for n in range(2):
        spread(0, 0, 0, 1, n, along_p(1))
        spread(0, 0, 0, 3, n, along_p(-1))
        send_q(0, n)
    for n in range(2):
        spread(0, 0, 0, 2, n, along_p(2))
    def pass_first(n):
        arrived(0, 1, n)
        send_q(1, n)
        arrived(0, 3, n)
        send_q(3, n)
        pass_on(0, n)

    pass_first(0)
    ring[2].wait_recv()
    forward(2, 3)
    ring[6].wait_recv()
    forward(6, 5)
    across(2)
    across(6)
    pass_first(1)
    for n in range(2):
        arrived(0, 2, n)
        send_q(2, n)
        spread(0, 2, 2, 2, n, along_q(2))
    for n in (14, 15, 16):
        loads[n].wait()
    for copy in swap:
        copy.wait_recv()

    def operands(start, count):
        rest = xs[start : start + count, 32:40, :].reshape(8 * count, 1024)
        main = [xs[start : start + count, 16 * h : 16 * h + 16, :].reshape(16 * count, 1024) for h in range(2)]
        return [jnp.concatenate([part, rest], axis=0) for part in main]

    def product(pair, w_lo, w_hi):
        lo, hi = dot_nt(pair[0], w_lo), dot_nt(pair[1], w_hi)
        main = lo.shape[0] // 3 * 2
        rest_lo, rest_hi = lo[main:, :], hi[main:, :]
        count = rest_lo.shape[0]
        top = iota((count, 1), 0) % 8 < 4
        rest = jnp.where(top, rest_lo, pltpu.roll(rest_lo, 4, 0)) + jnp.where(
            top, pltpu.roll(rest_hi, count - 4, 0), rest_hi
        )
        return jnp.concatenate([lo[0:main, :] + hi[0:main, :], rest], axis=0)

    def column(start, count, lane):
        tiles = sc[start : start + count].astype(F32)
        main = jnp.concatenate([tiles[:, :, lane : lane + 1], tiles[:, :, lane + 2 : lane + 3]], axis=1)
        rest = tiles[:, :, lane + 4 : lane + 5]
        return jnp.concatenate([main.reshape(16 * count, 1), rest.reshape(8 * count, 1)], axis=0)

    def expert_rows(pair, start, count):
        gate, up = (product(pair, we[t, :, 0:1024], we[t, :, 1024:2048]) for t in range(2))
        return (silu(gate) * up * column(start, count, 0)).astype(BF16)

    def dense_rows(pair, start, count):
        gate, up = (product(pair, wd[t, 0], wd[t, 1]) for t in range(2))
        share = jnp.where(iota(gate.shape, 1) // 24 == column(start, count, 1).astype(jnp.int32), 1.0, 0.5)
        return (silu(gate) * up * (share / (1.0 + jnp.exp(-gate[:, 22:23])))).astype(BF16)

    own = operands(12, 4)
    own_e = expert_rows(own, 12, 4)
    for n in range(2):
        pass_on(1, n)
        pass_on(3, n)
    for n in range(2):
        for rp in range(4):
            for rq in (1, 3):
                if rp == 2 or PASS[rp] != 2 - rq:
                    arrived(rq, rp, n)
    near_e = expert_rows(operands(4, 8), 4, 8)
    for n in (3, 5):
        ring[n].wait_recv()
        across(n)
    for n in range(2):
        for rp in range(4):
            arrived(2, rp, n)
    far = operands(0, 4)
    far_e = expert_rows(far, 0, 4)
    for copy in cross.values():
        copy.wait_recv()
    far_d = dense_rows(far, 0, 4)

    def blocks(rows, start, count):
        return jnp.concatenate(
            [rows[16 * start : 16 * (start + count), :], rows[192 + 8 * start : 192 + 8 * (start + count), :]], axis=0
        )

    def down(hidden_e, hidden_d, start, count, then):
        main = 16 * count
        top = iota((8 * count, 1), 0) % 8 < 4
        for n in range(2):
            cols = slice(512 * n, 512 * n + 512)
            part = [
                dot(hidden_e, we[2, :, 1024 * h + 512 * n : 1024 * h + 512 * n + 512]) + dot(hidden_d, wd[2, h, :, cols])
                for h in range(2)
            ]
            for h in range(2):
                outs[start : start + count, 16 * h : 16 * h + 16, cols] = (
                    part[h][0:main, :].astype(BF16).reshape(count, 16, 512)
                )
            rest = jnp.where(top, part[0][main:, :], part[1][main:, :])
            outs[start : start + count, 32:40, cols] = rest.reshape(count, 8, 512).astype(BF16)
            then(n)

    back = {}

    def part(ref, rp, n):
        return ref.at[rp, :, pl.ds(512 * n, 512)]

    def part_rows(ref, rp, n):
        return ref[rp, :, 512 * n : 512 * n + 512].astype(F32)

    def send_far(n):
        back["far", n] = started(chunk(outs, 2, 2, n), part(opp_q, 2, n), along_q(2))
        for rp in (1, 3, 0):
            back[2, rp, n] = started(chunk(outs, 2, rp, n), part(opp_q, rp, n), along_q(-PASS[rp]))

    def send_back(rq, rp, n):
        device = along_q(-1 if rq == 1 else 1)
        back[rq, rp, n] = started(chunk(outs, rq, rp, n), part(fin_q.at[rq // 2], rp, n), device)

    def send_near(n):
        for rq, rp in ((1, 2), (3, 2), (1, 1), (3, 1), (1, 3), (3, 3), (1, 0), (3, 0)):
            if rp == 2 or PASS[rp] != 2 - rq:
                send_back(rq, rp, n)

    down(far_e, far_d, 0, 4, send_far)
    rest_d = dense_rows(operands(4, 12), 4, 12)
    down(near_e, blocks(rest_d, 0, 8), 4, 8, send_near)
    down(own_e, blocks(rest_d, 8, 4), 12, 4, lambda n: None)
    for n in range(2):
        for rp in (1, 3, 0):
            rq = 2 - PASS[rp]
            at = 4 * AT[rq] + rp
            back[2, rp, n].wait_recv()
            both = part_rows(outs, at, n) + part_rows(opp_q, rp, n)
            outs[at, :, 512 * n : 512 * n + 512] = both.astype(BF16)
            send_back(rq, rp, n)

    total = {}

    def sum_q(rp, n):
        for rq in (1, 3):
            back[rq, rp, n].wait_recv()
        own_part = part_rows(outs, 4 * AT[0] + rp, n)
        total[rp, n] = own_part + part_rows(fin_q.at[0], rp, n) + part_rows(fin_q.at[1], rp, n)

    def send_p(slot, rp, n, by):
        tsend[slot, :, 512 * n : 512 * n + 512] = total[rp, n].astype(BF16)
        back["p", slot, n] = started(part(tsend, slot, n), part(fin_p, slot, n), along_p(by))

    for n in range(2):
        sum_q(2, n)
        back["far", n].wait_recv()
        total[2, n] = total[2, n] + part_rows(opp_q, 2, n)
        send_p(0, 2, n, 2)
    for n in range(2):
        sum_q(1, n)
        send_p(1, 1, n, -1)
        sum_q(3, n)
        send_p(2, 3, n, 1)
    for n in range(2):
        sum_q(0, n)
    ends = []
    for n in range(2):
        for slot in range(3):
            back["p", slot, n].wait_recv()
        ends.append(total[0, n] + part_rows(fin_p, 0, n) + part_rows(fin_p, 1, n) + part_rows(fin_p, 2, n))
    summed = jnp.concatenate(ends, axis=1).astype(BF16)

    for h in range(2):
        rbuf[h] = dot(pack_matrix(iota((32, 40), 1), iota((32, 40), 0), h), summed).astype(BF16)

    def ret_copy(j, h, device):
        d = 4 * c + j
        return pltpu.make_async_remote_copy(
            src_ref=rbuf.at[h, pl.ds(SLOT * j, SLOT)],
            dst_ref=ret.at[pl.ds(pl.multiple_of(SLOT * d, SLOT), SLOT)],
            send_sem=ret_send.at[2 * j + h],
            recv_sem=ret_recv.at[d],
            device_id=device,
            device_id_type=MESH,
        )

    def ret_device(j, h):
        return {**along_z(4 * c + j), "tp": h}

    def ret_each(act):
        @pl.when(first)
        def _():
            for j in (3, 2, 1):
                for h in range(2):
                    act(ret_copy(j, h, ret_device(j, h)))
            act(ret_copy(0, 1, {"tp": 1}))

        @pl.when(jnp.logical_not(first))
        def _():
            for j in range(4):
                for h in range(2):
                    act(ret_copy(j, h, ret_device(j, h)))

    ret_each(lambda copy: copy.start())

    @pl.when(first)
    def _():
        ret[0:SLOT, :] = rbuf[0, 0:SLOT, :]

    def ret_wait(d):
        pltpu.make_async_remote_copy(
            src_ref=rbuf.at[0, pl.ds(0, SLOT)],
            dst_ref=ret.at[pl.ds(SLOT * d, SLOT)],
            send_sem=ret_send.at[0],
            recv_sem=ret_recv.at[d],
            device_id=partner,
            device_id_type=MESH,
        ).wait_recv()

    after_own, _ = halves(after[:, 0:1024], after[:, 1024:2048])
    for d in range(1, 8):
        ret_wait(d)

    @pl.when(jnp.logical_not(first))
    def _():
        ret_wait(0)

    mixed[...] = (after_own + dot_tn(chosen.astype(BF16), ret[...])).astype(BF16)

    for copy in sent:
        copy.wait_send()
    for j in (1, 2, 3):
        moved[j].wait_send()

    @pl.when(jnp.logical_not(first))
    def _():
        moved[0].wait_send()

    ret_each(lambda copy: copy.wait_send())
    assert used[0] <= COPIES


def body(
    tokens,
    state,
    norm_mix,
    w_query,
    w_key,
    w_value,
    w_out,
    norm_ffn,
    gate_vector,
    dense_gate,
    dense_up,
    dense_down,
    exp_gate,
    exp_up,
    exp_down,
    routes,
    route_w,
):
    vmem = pl.BlockSpec(memory_space=pltpu.VMEM)
    hbm = pl.BlockSpec(memory_space=pltpu.HBM)

    def buf(*shape, dtype=BF16):
        return pltpu.VMEM(shape, dtype)

    return pl.pallas_call(
        kernel,
        out_shape=(
            pltpu.VMEM(tokens.shape, tokens.dtype),
            pltpu.VMEM(state.shape, state.dtype),
        ),
        in_specs=[hbm] * 17,
        out_specs=(vmem, vmem),
        scratch_shapes=[
            buf(16, 1024),
            buf(1, 2048, dtype=F32),
            buf(1, 1024, dtype=F32),
            buf(8, 128),
            buf(2, 16, dtype=jnp.int32),
            buf(2, 16),
            buf(22, 1024),
            buf(22, 1024),
            buf(22, 1024),
            buf(2048, 256),
            buf(2048, 256),
            buf(2048, 256),
            buf(256, 2048),
            buf(16, 256, dtype=F32),
            buf(16, 1024),
            buf(1, 1024, dtype=F32),
            buf(16, 2048),
            buf(16, 2048),
            buf(3, 176, 2048),
            buf(3, 2, 168, 1024),
            buf(32, 2176),
            buf(32, 2176),
            buf(16, 40, 1024),
            buf(16, 8, 128),
            buf(16, 40, 1024),
            buf(4, 40, 1024),
            buf(2, 4, 40, 1024),
            buf(3, 40, 1024),
            buf(3, 40, 1024),
            buf(2, 32, 1024),
            buf(64, 1024),
            pltpu.SemaphoreType.DMA((17,)),
            pltpu.SemaphoreType.DMA((COPIES,)),
            pltpu.SemaphoreType.DMA((COPIES,)),
            pltpu.SemaphoreType.DMA((8,)),
            pltpu.SemaphoreType.DMA((8,)),
            pltpu.SemaphoreType.REGULAR((4,)),
        ],
        compiler_params=pltpu.CompilerParams(collective_id=0, has_side_effects=True, vmem_limit_bytes=56 * 1024 * 1024),
        name="layer",
    )(
        *(
            pltpu.with_memory_space_constraint(operand, pltpu.HBM)
            for operand in (
                tokens,
                norm_mix.reshape(1, -1),
                norm_ffn.reshape(1, -1),
                gate_vector.reshape(8, 128),
                routes.T,
                route_w.T,
                dense_gate.T,
                dense_up.T,
                dense_down,
                state,
                w_query,
                w_key,
                w_value,
                w_out,
                exp_gate[0].T,
                exp_up[0].T,
                exp_down[0],
            )
        )
    )


def solution(mesh):
    finer = Mesh(mesh.devices.reshape(8, 4, 4, mesh.shape["tp"]), (*EP, "tp"))
    in_specs = (
        P(EP, "tp"),
        P(EP, "tp", None, None),
        P(),
        P(None, "tp"),
        P(None, "tp"),
        P(None, "tp"),
        P("tp", None),
        P("tp"),
        P("tp"),
        P("tp", EP),
        P("tp", EP),
        P(EP, "tp"),
        P(EP, None, "tp"),
        P(EP, None, "tp"),
        P(EP, "tp", None),
        P(EP, None),
        P(EP, None),
    )
    out_specs = (P(EP, "tp"), P(EP, "tp", None, None))
    return jax.shard_map(body, mesh=finer, in_specs=in_specs, out_specs=out_specs, check_vma=False)
```

```python
import jax
import jax.numpy as jnp
from jax import lax
from jax.experimental import pallas as pl
from jax.experimental.pallas import tpu as pltpu
from jax.sharding import Mesh
from jax.sharding import PartitionSpec as P

EP = ("ep_0", "ep_1", "ep_2")
Z, Y, X = EP
MESH = pl.DeviceIdType.MESH
SLOT = 8
CAP = 5
F32 = jnp.float32
BF16 = jnp.bfloat16
epsilon = 1e-06
COPIES = 112
AT = {2: 0, 1: 1, 3: 2, 0: 3}
PASS = {0: -1, 1: 1, 3: -1}


def iota(shape, dim):
    return lax.broadcasted_iota(jnp.int32, shape, dim)


def dot(a, b):
    return jnp.dot(a, b, preferred_element_type=F32)


def dot_nt(a, b):
    return lax.dot_general(a, b, (((1,), (1,)), ((), ())), preferred_element_type=F32)


def dot_tn(a, b):
    return lax.dot_general(a, b, (((0,), (0,)), ((), ())), preferred_element_type=F32)


def silu(v):
    return v / (1.0 + jnp.exp(-v))


def pack_matrix(row, col, half):
    main = row < 32
    slot = jnp.where(main, row % 16, 16 + row % 4)
    part = jnp.where(main, row // 16, (row - 32) // 4)
    return jnp.where((part == half) & (col == slot // CAP * SLOT + slot % CAP), 1.0, 0.0).astype(BF16)


def kernel(
    tokens_h,
    norm_mix_h,
    norm_ffn_h,
    gate_vec_h,
    routes_h,
    route_w_h,
    dgate_h,
    dup_h,
    ddown_h,
    state,
    w_query,
    w_key,
    w_value,
    w_out,
    egate,
    eup,
    edown,
    mixed,
    st,
    tokens,
    norm_mix,
    norm_ffn,
    gate_vec,
    routes,
    route_w,
    dgate,
    dup,
    ddown,
    wq,
    wk,
    wv,
    wo,
    read,
    tok_p,
    nf_p,
    mix_o,
    mix_p,
    we,
    wd,
    disp,
    zrecv,
    xs,
    sc,
    outs,
    opp_q,
    fin_q,
    tsend,
    fin_p,
    rbuf,
    ret,
    local_sem,
    send_sem,
    recv_sem,
    ret_send,
    ret_recv,
    known,
):
    z, y, x, c = (lax.axis_index(a) for a in (Z, Y, X, "tp"))
    first = c == 0
    used = [0]

    def wrap(value, size):
        return lax.rem(value + size, size)

    def along_z(by):
        return {Z: wrap(z + by, 8)}

    def along_p(by):
        return {X: wrap(x + by * (1 - c), 4), Y: wrap(y + by * c, 4)}

    def along_q(by):
        return {X: wrap(x + by * c, 4), Y: wrap(y + by * (1 - c), 4)}

    partner = {"tp": 1 - c}

    def remote(src, dst, device):
        n = used[0]
        used[0] += 1
        return pltpu.make_async_remote_copy(
            src_ref=src,
            dst_ref=dst,
            send_sem=send_sem.at[n],
            recv_sem=recv_sem.at[n],
            device_id=device,
            device_id_type=MESH,
        )

    sent = []

    def started(src, dst, device):
        copy = remote(src, dst, device)
        copy.start()
        sent.append(copy)
        return copy

    def halves(own, other):
        return jnp.where(first, own, other), jnp.where(first, other, own)

    def as_row(ref):
        rows = ref[...].astype(F32)
        return jnp.concatenate([rows[i : i + 1, :] for i in range(8)], axis=1)

    loads = {}
    for n, (src, dst) in enumerate(
        [
            (tokens_h, tokens),
            (norm_ffn_h, norm_ffn),
            (dgate_h, dgate),
            (dup_h, dup),
            (ddown_h, ddown),
            (gate_vec_h, gate_vec),
            (norm_mix_h, norm_mix),
            (routes_h, routes),
            (route_w_h, route_w),
            (w_query, wq),
            (w_key, wk),
            (w_value, wv),
            (state, st),
            (w_out, wo),
            (egate, we.at[0, pl.ds(0, 88)]),
            (eup, we.at[1, pl.ds(0, 88)]),
            (edown, we.at[2, pl.ds(0, 88)]),
        ]
    ):
        loads[n] = pltpu.make_async_copy(src, dst, local_sem.at[n])
        loads[n].start()

    barrier = pltpu.get_barrier_semaphore()
    peers = [partner]
    for by in (1, -1):
        peers += [along_z(by), along_z(2 * by), along_p(by), along_q(by)]
    for peer in peers:
        pl.semaphore_signal(barrier, inc=1, device_id=peer, device_id_type=MESH)

    for n in range(9):
        loads[n].wait()
    tail = jnp.zeros((2, 1024), F32)
    gate_tail = jnp.concatenate([as_row(gate_vec), tail[0:1, :]], axis=0)
    for t, (ref, end) in enumerate(((dgate, gate_tail), (dup, tail), (ddown, tail))):
        block = jnp.concatenate([ref[...].astype(F32), end], axis=0)
        wd[t, pl.ds(c, 1), pl.ds(0, 24), :] = block.astype(BF16)[None]

    pl.semaphore_wait(barrier, len(peers))

    def tell(n, device):
        pl.semaphore_signal(known.at[n], inc=1, device_id=device, device_id_type=MESH)

    def hear(n):
        pl.semaphore_wait(known.at[n], 1)

    tell(0, along_z(2))
    tell(1, along_z(-2))
    tell(2, along_p(1))
    tell(3, along_q(1))

    pair = [started(tokens, tok_p, partner), started(norm_ffn, nf_p, partner)]

    def wd_slot(n):
        return wd.at[:, pl.ds(c, 1), pl.ds(24 * (n - (n > 4)), 24), :]

    ring, cross = {}, {}

    def forward(source, target):
        ring[target] = started(wd_slot(source), wd_slot(target), along_z(1 if target < 4 else -1))

    def across(n):
        cross[n] = started(wd_slot(n), wd_slot(n), partner)

    forward(0, 1)
    forward(0, 7)
    swap = [started(src, we.at[t, pl.ds(88, 88)], partner) for t, src in enumerate((egate, eup, edown))]
    across(0)

    for copy in pair:
        copy.wait_recv()
    lo, hi = halves(tokens[...].astype(F32), tok_p[...].astype(F32))
    full = jnp.concatenate([lo, hi], axis=1)
    mean = jnp.sum(full * full, axis=1, keepdims=True) / 2048.0
    normed = (full * lax.rsqrt(mean + epsilon) * norm_mix[...]).astype(BF16)
    for n in (9, 10, 11):
        loads[n].wait()
    query = dot(normed, wq[...]).astype(BF16).astype(F32)
    key = dot(normed, wk[...]).astype(BF16).astype(F32) * 128 ** (-0.5)
    value = dot(normed, wv[...]).astype(BF16).astype(F32)
    blank = jnp.zeros((112, 256), F32)
    query_t = jnp.concatenate([query, blank], axis=0).T
    key_t = jnp.concatenate([key, blank], axis=0).T
    loads[12].wait()
    decay = [jnp.where(first, 1.0 - 2.0 ** (-3.0 - 2.0 * h), 1.0 - 2.0 ** (-7.0 - 2.0 * h)) for h in range(2)]
    for h in range(2):
        span = slice(128 * h, 128 * h + 128)
        for s in range(16):
            read[s : s + 1, span] = jnp.sum(query_t[span, s : s + 1] * st[s, h], axis=0, keepdims=True)
    heads = []
    for h in range(2):
        span = slice(128 * h, 128 * h + 128)
        met = jnp.sum(query[:, span] * key[:, span], axis=1, keepdims=True)
        part = decay[h] * read[:, span] + met * value[:, span]
        centre = jnp.mean(part, axis=1, keepdims=True)
        spread = jnp.mean(jnp.square(part - centre), axis=1, keepdims=True)
        heads.append(((part - centre) * lax.rsqrt(spread + epsilon)).astype(BF16))
    loads[13].wait()
    mix = dot(heads[0], wo[0:128, :]) + dot(heads[1], wo[128:256, :])
    mix_o[...] = mix.astype(BF16)
    mix_copy = started(mix_o, mix_p, partner)

    block = iota((64, 16), 0)
    expert = lax.rem(z - block // SLOT + 8, 8)
    hit0 = jnp.where(routes[0:1, :] == expert, 1.0, 0.0)
    hit1 = jnp.where(routes[1:2, :] == expert, 1.0, 0.0)
    member = hit0 + hit1
    before = jnp.where(iota((16, 16), 0) < iota((16, 16), 1), 1.0, 0.0).astype(BF16)
    place = dot(member.astype(BF16), before)
    chosen = jnp.where(place == (block % SLOT).astype(F32), member, 0.0)
    weights = route_w[...].astype(F32)
    slot_w = jnp.sum(chosen * (hit0 * weights[0:1, :] + hit1 * weights[1:2, :]), axis=1, keepdims=True)
    other = jnp.where(hit0 > 0.0, routes[1:2, :], routes[0:1, :])
    absent = lax.rem(expert - other + 12, 8)
    absent = jnp.where(absent > 4, absent - 1, absent).astype(F32)
    slot_absent = jnp.sum(chosen * absent, axis=1, keepdims=True)
    extra = jnp.where(iota((64, 128), 1) % 2 == 0, slot_w, slot_absent)
    extra = jnp.where(first, extra[0:32, :], extra[32:64, :]).astype(BF16)
    mine = jnp.where(first, chosen[0:32, :], chosen[32:64, :]).astype(BF16)

    mix_copy.wait_recv()
    after = (full + (mix_o[...].astype(F32) + mix_p[...].astype(F32))).astype(BF16).astype(F32)
    mean2 = jnp.sum(after * after, axis=1, keepdims=True) / 2048.0
    nf_lo, nf_hi = halves(norm_ffn[...], nf_p[...])
    normed2 = (after * lax.rsqrt(mean2 + epsilon) * jnp.concatenate([nf_lo, nf_hi], axis=1)).astype(BF16)

    hear(0)
    hear(1)
    rows = dot(mine, normed2)
    disp[:, 2048:2176] = extra
    disp[:, 0:2048] = rows.astype(BF16)
    moved = []
    for j in range(4):
        part = pl.ds(SLOT * j, SLOT)
        moved.append(remote(disp.at[part], zrecv.at[part], along_z(-(4 * c + j))))

    @pl.when(first)
    def _():
        for j in (3, 2, 1):
            moved[j].start()
        zrecv[0:SLOT, :] = disp[0:SLOT, :]

    @pl.when(jnp.logical_not(first))
    def _():
        for j in range(4):
            moved[j].start()

    for h in range(2):
        span = slice(128 * h, 128 * h + 128)
        for s in range(16):
            st[s, h] = decay[h] * st[s, h] + key_t[span, s : s + 1] * value[s : s + 1, span]

    for j in (1, 2, 3):
        moved[j].wait_recv()

    @pl.when(jnp.logical_not(first))
    def _():
        moved[0].wait_recv()

    ring[1].wait_recv()
    forward(1, 2)
    ring[7].wait_recv()
    forward(7, 6)
    across(1)
    across(7)
    def cell(ref, rq, rp):
        return ref.at[4 * AT[rq] + rp]

    def cell_rows(ref, rq, rp):
        return ref[4 * AT[rq] + rp].astype(F32)

    def set_rows(ref, rq, rp, rows):
        ref[4 * AT[rq] + rp] = rows.astype(BF16)

    row, col = iota((40, 32), 0), iota((40, 32), 1)
    packed = dot(pack_matrix(row, col, 0), zrecv[:, 0:1024]) + dot(pack_matrix(row, col, 1), zrecv[:, 1024:2048])
    set_rows(xs, 0, 0, packed)
    lane8, row8, col8 = iota((8, 128), 1), iota((8, 32), 0), iota((8, 32), 1)

    def scalars(slot):
        pick = jnp.where(col8 == slot // CAP * SLOT + slot % CAP, 1.0, 0.0).astype(BF16)
        return dot(pick, zrecv[:, 2048:2176])

    packed_sc = jnp.where(
        lane8 < 2, scalars(row8), jnp.where(lane8 < 4, scalars(row8 + 8), scalars(16 + row8 % 4))
    )
    set_rows(sc, 0, 0, packed_sc)

    got = {}

    def chunk(ref, rq, rp, n):
        return ref.at[4 * AT[rq] + rp, :, pl.ds(512 * n, 512)]

    def spread(from_q, from_p, to_q, to_p, n, device):
        got[to_q, to_p, n] = started(chunk(xs, from_q, from_p, n), chunk(xs, to_q, to_p, n), device)
        if n == 0:
            got[to_q, to_p, 2] = started(cell(sc, from_q, from_p), cell(sc, to_q, to_p), device)

    def arrived(rq, rp, n):
        got[rq, rp, n].wait_recv()
        if n == 0:
            got[rq, rp, 2].wait_recv()

    def send_q(rp, n):
        spread(0, rp, 1, rp, n, along_q(1))
        spread(0, rp, 3, rp, n, along_q(-1))

    def pass_on(rp, n):
        by = PASS[rp]
        arrived(2 - by, rp, n)
        spread(2 - by, rp, 2, rp, n, along_q(by))

    hear(2)
    hear(3)
    for n in range(2):
        spread(0, 0, 0, 1, n, along_p(1))
        spread(0, 0, 0, 3, n, along_p(-1))
        send_q(0, n)
    for n in range(2):
        spread(0, 0, 0, 2, n, along_p(2))
    def pass_first(n):
        arrived(0, 1, n)
        send_q(1, n)
        arrived(0, 3, n)
        send_q(3, n)
        pass_on(0, n)

    pass_first(0)
    ring[2].wait_recv()
    forward(2, 3)
    ring[6].wait_recv()
    forward(6, 5)
    across(2)
    across(6)
    pass_first(1)
    for n in range(2):
        arrived(0, 2, n)
        send_q(2, n)
        spread(0, 2, 2, 2, n, along_q(2))
    for n in (14, 15, 16):
        loads[n].wait()
    for copy in swap:
        copy.wait_recv()

    def operands(start, count):
        rest = xs[start : start + count, 32:40, :].reshape(8 * count, 1024)
        main = [xs[start : start + count, 16 * h : 16 * h + 16, :].reshape(16 * count, 1024) for h in range(2)]
        return [jnp.concatenate([part, rest], axis=0) for part in main]

    def product(pair, w_lo, w_hi):
        lo, hi = dot_nt(pair[0], w_lo), dot_nt(pair[1], w_hi)
        main = lo.shape[0] // 3 * 2
        rest_lo, rest_hi = lo[main:, :], hi[main:, :]
        count = rest_lo.shape[0]
        top = iota((count, 1), 0) % 8 < 4
        rest = jnp.where(top, rest_lo, pltpu.roll(rest_lo, 4, 0)) + jnp.where(
            top, pltpu.roll(rest_hi, count - 4, 0), rest_hi
        )
        return jnp.concatenate([lo[0:main, :] + hi[0:main, :], rest], axis=0)

    def column(start, count, lane):
        tiles = sc[start : start + count].astype(F32)
        main = jnp.concatenate([tiles[:, :, lane : lane + 1], tiles[:, :, lane + 2 : lane + 3]], axis=1)
        rest = tiles[:, :, lane + 4 : lane + 5]
        return jnp.concatenate([main.reshape(16 * count, 1), rest.reshape(8 * count, 1)], axis=0)

    def expert_rows(pair, start, count):
        gate, up = (product(pair, we[t, :, 0:1024], we[t, :, 1024:2048]) for t in range(2))
        return (silu(gate) * up * column(start, count, 0)).astype(BF16)

    def dense_rows(pair, start, count):
        gate, up = (product(pair, wd[t, 0], wd[t, 1]) for t in range(2))
        share = jnp.where(iota(gate.shape, 1) // 24 == column(start, count, 1).astype(jnp.int32), 1.0, 0.5)
        return (silu(gate) * up * (share / (1.0 + jnp.exp(-gate[:, 22:23])))).astype(BF16)

    own = operands(12, 4)
    own_e = expert_rows(own, 12, 4)
    for n in range(2):
        pass_on(1, n)
        pass_on(3, n)
    for n in range(2):
        for rp in range(4):
            for rq in (1, 3):
                if rp == 2 or PASS[rp] != 2 - rq:
                    arrived(rq, rp, n)
    near_e = expert_rows(operands(4, 8), 4, 8)
    for n in (3, 5):
        ring[n].wait_recv()
        across(n)
    for n in range(2):
        for rp in range(4):
            arrived(2, rp, n)
    far = operands(0, 4)
    far_e = expert_rows(far, 0, 4)
    for copy in cross.values():
        copy.wait_recv()
    far_d = dense_rows(far, 0, 4)

    def blocks(rows, start, count):
        return jnp.concatenate(
            [rows[16 * start : 16 * (start + count), :], rows[192 + 8 * start : 192 + 8 * (start + count), :]], axis=0
        )

    def down(hidden_e, hidden_d, start, count, then):
        main = 16 * count
        top = iota((8 * count, 1), 0) % 8 < 4
        for n in range(2):
            cols = slice(512 * n, 512 * n + 512)
            part = [
                dot(hidden_e, we[2, :, 1024 * h + 512 * n : 1024 * h + 512 * n + 512]) + dot(hidden_d, wd[2, h, :, cols])
                for h in range(2)
            ]
            for h in range(2):
                outs[start : start + count, 16 * h : 16 * h + 16, cols] = (
                    part[h][0:main, :].astype(BF16).reshape(count, 16, 512)
                )
            rest = jnp.where(top, part[0][main:, :], part[1][main:, :])
            outs[start : start + count, 32:40, cols] = rest.reshape(count, 8, 512).astype(BF16)
            then(n)

    back = {}

    def part(ref, rp, n):
        return ref.at[rp, :, pl.ds(512 * n, 512)]

    def part_rows(ref, rp, n):
        return ref[rp, :, 512 * n : 512 * n + 512].astype(F32)

    def send_far(n):
        back["far", n] = started(chunk(outs, 2, 2, n), part(opp_q, 2, n), along_q(2))
        for rp in (1, 3, 0):
            back[2, rp, n] = started(chunk(outs, 2, rp, n), part(opp_q, rp, n), along_q(-PASS[rp]))

    def send_back(rq, rp, n):
        device = along_q(-1 if rq == 1 else 1)
        back[rq, rp, n] = started(chunk(outs, rq, rp, n), part(fin_q.at[rq // 2], rp, n), device)

    def send_near(n):
        for rq, rp in ((1, 2), (3, 2), (1, 1), (3, 1), (1, 3), (3, 3), (1, 0), (3, 0)):
            if rp == 2 or PASS[rp] != 2 - rq:
                send_back(rq, rp, n)

    down(far_e, far_d, 0, 4, send_far)
    rest_d = dense_rows(operands(4, 12), 4, 12)
    down(near_e, blocks(rest_d, 0, 8), 4, 8, send_near)
    down(own_e, blocks(rest_d, 8, 4), 12, 4, lambda n: None)
    for n in range(2):
        for rp in (1, 3, 0):
            rq = 2 - PASS[rp]
            at = 4 * AT[rq] + rp
            back[2, rp, n].wait_recv()
            both = part_rows(outs, at, n) + part_rows(opp_q, rp, n)
            outs[at, :, 512 * n : 512 * n + 512] = both.astype(BF16)
            send_back(rq, rp, n)

    total = {}

    def sum_q(rp, n):
        for rq in (1, 3):
            back[rq, rp, n].wait_recv()
        own_part = part_rows(outs, 4 * AT[0] + rp, n)
        total[rp, n] = own_part + part_rows(fin_q.at[0], rp, n) + part_rows(fin_q.at[1], rp, n)

    def send_p(slot, rp, n, by):
        tsend[slot, :, 512 * n : 512 * n + 512] = total[rp, n].astype(BF16)
        back["p", slot, n] = started(part(tsend, slot, n), part(fin_p, slot, n), along_p(by))

    for n in range(2):
        sum_q(2, n)
        back["far", n].wait_recv()
        total[2, n] = total[2, n] + part_rows(opp_q, 2, n)
        send_p(0, 2, n, 2)
    for n in range(2):
        sum_q(1, n)
        send_p(1, 1, n, -1)
        sum_q(3, n)
        send_p(2, 3, n, 1)
    for n in range(2):
        sum_q(0, n)
    ends = []
    for n in range(2):
        for slot in range(3):
            back["p", slot, n].wait_recv()
        ends.append(total[0, n] + part_rows(fin_p, 0, n) + part_rows(fin_p, 1, n) + part_rows(fin_p, 2, n))
    summed = jnp.concatenate(ends, axis=1).astype(BF16)

    for h in range(2):
        rbuf[h] = dot(pack_matrix(iota((32, 40), 1), iota((32, 40), 0), h), summed).astype(BF16)

    def ret_copy(j, h, device):
        d = 4 * c + j
        return pltpu.make_async_remote_copy(
            src_ref=rbuf.at[h, pl.ds(SLOT * j, SLOT)],
            dst_ref=ret.at[pl.ds(pl.multiple_of(SLOT * d, SLOT), SLOT)],
            send_sem=ret_send.at[2 * j + h],
            recv_sem=ret_recv.at[d],
            device_id=device,
            device_id_type=MESH,
        )

    def ret_device(j, h):
        return {**along_z(4 * c + j), "tp": h}

    def ret_each(act):
        @pl.when(first)
        def _():
            for j in (3, 2, 1):
                for h in range(2):
                    act(ret_copy(j, h, ret_device(j, h)))
            act(ret_copy(0, 1, {"tp": 1}))

        @pl.when(jnp.logical_not(first))
        def _():
            for j in range(4):
                for h in range(2):
                    act(ret_copy(j, h, ret_device(j, h)))

    ret_each(lambda copy: copy.start())

    @pl.when(first)
    def _():
        ret[0:SLOT, :] = rbuf[0, 0:SLOT, :]

    def ret_wait(d):
        pltpu.make_async_remote_copy(
            src_ref=rbuf.at[0, pl.ds(0, SLOT)],
            dst_ref=ret.at[pl.ds(SLOT * d, SLOT)],
            send_sem=ret_send.at[0],
            recv_sem=ret_recv.at[d],
            device_id=partner,
            device_id_type=MESH,
        ).wait_recv()

    after_own, _ = halves(after[:, 0:1024], after[:, 1024:2048])
    for d in range(1, 8):
        ret_wait(d)

    @pl.when(jnp.logical_not(first))
    def _():
        ret_wait(0)

    mixed[...] = (after_own + dot_tn(chosen.astype(BF16), ret[...])).astype(BF16)

    for copy in sent:
        copy.wait_send()
    for j in (1, 2, 3):
        moved[j].wait_send()

    @pl.when(jnp.logical_not(first))
    def _():
        moved[0].wait_send()

    ret_each(lambda copy: copy.wait_send())
    assert used[0] <= COPIES


def leave(mixed, state, mixed_out, state_out, sem):
    copies = [pltpu.make_async_copy(mixed, mixed_out, sem.at[8])]
    for n in range(8):
        part = pl.ds(2 * n, 2)
        copies.append(pltpu.make_async_copy(state.at[part], state_out.at[part], sem.at[n]))
    for copy in copies:
        copy.start()
    for copy in copies:
        copy.wait()


def body(
    tokens,
    state,
    norm_mix,
    w_query,
    w_key,
    w_value,
    w_out,
    norm_ffn,
    gate_vector,
    dense_gate,
    dense_up,
    dense_down,
    exp_gate,
    exp_up,
    exp_down,
    routes,
    route_w,
):
    vmem = pl.BlockSpec(memory_space=pltpu.VMEM)
    hbm = pl.BlockSpec(memory_space=pltpu.HBM)

    def buf(*shape, dtype=BF16):
        return pltpu.VMEM(shape, dtype)

    results = pl.pallas_call(
        kernel,
        out_shape=(
            pltpu.VMEM(tokens.shape, tokens.dtype),
            pltpu.VMEM(state.shape, state.dtype),
        ),
        in_specs=[hbm] * 17,
        out_specs=(vmem, vmem),
        scratch_shapes=[
            buf(16, 1024),
            buf(1, 2048, dtype=F32),
            buf(1, 1024, dtype=F32),
            buf(8, 128),
            buf(2, 16, dtype=jnp.int32),
            buf(2, 16),
            buf(22, 1024),
            buf(22, 1024),
            buf(22, 1024),
            buf(2048, 256),
            buf(2048, 256),
            buf(2048, 256),
            buf(256, 2048),
            buf(16, 256, dtype=F32),
            buf(16, 1024),
            buf(1, 1024, dtype=F32),
            buf(16, 2048),
            buf(16, 2048),
            buf(3, 176, 2048),
            buf(3, 2, 168, 1024),
            buf(32, 2176),
            buf(32, 2176),
            buf(16, 40, 1024),
            buf(16, 8, 128),
            buf(16, 40, 1024),
            buf(4, 40, 1024),
            buf(2, 4, 40, 1024),
            buf(3, 40, 1024),
            buf(3, 40, 1024),
            buf(2, 32, 1024),
            buf(64, 1024),
            pltpu.SemaphoreType.DMA((17,)),
            pltpu.SemaphoreType.DMA((COPIES,)),
            pltpu.SemaphoreType.DMA((COPIES,)),
            pltpu.SemaphoreType.DMA((8,)),
            pltpu.SemaphoreType.DMA((8,)),
            pltpu.SemaphoreType.REGULAR((4,)),
        ],
        compiler_params=pltpu.CompilerParams(collective_id=0, has_side_effects=True, vmem_limit_bytes=56 * 1024 * 1024),
        name="layer",
    )(
        *(
            pltpu.with_memory_space_constraint(operand, pltpu.HBM)
            for operand in (
                tokens,
                norm_mix.reshape(1, -1),
                norm_ffn.reshape(1, -1),
                gate_vector.reshape(8, 128),
                routes.T,
                route_w.T,
                dense_gate.T,
                dense_up.T,
                dense_down,
                state,
                w_query,
                w_key,
                w_value,
                w_out,
                exp_gate[0].T,
                exp_up[0].T,
                exp_down[0],
            )
        )
    )
    return pl.pallas_call(
        leave,
        out_shape=(
            jax.ShapeDtypeStruct(tokens.shape, tokens.dtype),
            jax.ShapeDtypeStruct(state.shape, state.dtype),
        ),
        in_specs=[vmem, vmem],
        out_specs=(hbm, hbm),
        scratch_shapes=[pltpu.SemaphoreType.DMA((9,))],
        name="leave",
        compiler_params=pltpu.CompilerParams(vmem_limit_bytes=4 * 1024 * 1024),
    )(*(pltpu.with_memory_space_constraint(result, pltpu.VMEM) for result in results))


def solution(mesh):
    finer = Mesh(mesh.devices.reshape(8, 4, 4, mesh.shape["tp"]), (*EP, "tp"))
    in_specs = (
        P(EP, "tp"),
        P(EP, "tp", None, None),
        P(),
        P(None, "tp"),
        P(None, "tp"),
        P(None, "tp"),
        P("tp", None),
        P("tp"),
        P("tp"),
        P("tp", EP),
        P("tp", EP),
        P(EP, "tp"),
        P(EP, None, "tp"),
        P(EP, None, "tp"),
        P(EP, "tp", None),
        P(EP, None),
        P(EP, None),
    )
    out_specs = (P(EP, "tp"), P(EP, "tp", None, None))
    return jax.shard_map(body, mesh=finer, in_specs=in_specs, out_specs=out_specs, check_vma=False)
```
